32 devices in a mesh: kv: 8 (over z, y), tp: 4 (over x, core).
Axes of the slice: x: 2, y: 2, z: 4, core: 2. Of those that a mesh axis runs over, the one named last changes fastest.
Arguments:
- queries: bfloat16 [2, 3072, 1024], P(None, 'kv', 'tp'), may hold values from -112 to 112
- key_states: bfloat16 [2, 3072, 256], P(None, 'kv', 'tp'), may hold values from -4 to 4
- value_states: bfloat16 [2, 3072, 256], P(None, 'kv', 'tp'), may hold values from -6 to 6
- cotangent: bfloat16 [2, 3072, 1024], P(None, 'kv', 'tp'), may hold values from -6 to 6
- gate_logits: float32 [2, 3072, 16], P(None, 'kv', 'tp'), may hold values from -6 to 6
- layer_input: bfloat16 [2, 3072, 4096], P(None, ('kv', 'tp')), may hold values from -6 to 6
- chosen: int32 [2, 48, 4, 16], P(None, 'kv', 'tp'), may hold values from 0 to 47, as said below
Outputs:
- query_grad: bfloat16 [2, 3072, 1024], P(None, 'kv', 'tp')
- key_grad: bfloat16 [2, 3072, 256], P(None, 'kv', 'tp')
- value_grad: bfloat16 [2, 3072, 256], P(None, 'kv', 'tp')
- value_weight_grad: float32 [4096, 256], P(('kv', 'tp'))
The draws below stay inside these ranges and needn't reach their ends.
Inputs may be any that keep to these rules, and one draw needn't show every extreme that they name: `chosen`: for each sequence, query block b and key head, the 16 entries are distinct blocks; they include b itself and block 0; blocks after b hold only keys after all of the block's queries. Taking the 6 query blocks of one index of kv together (aligned), one sequence and one key head, at most 2 distinct blocks held by any one earlier index of kv are named, and some index reaches 2.
All inputs are finite; a program needn't handle non-finite values.
Results may differ from the reference program's by a relative error of at most 0.0058.
Values may be sent and summed in bfloat16 or wider, within the bound.
A program may use at most 128 MiB of HBM per device.

```python
import jax
import jax.numpy as jnp
from jax import lax

D = 4096
H = 16
KVH = 4
HD = 64
BLK = 64
TOPK = 16
MOST = 2
SEQS = 2
BPD = 6
SEQ = 3072
NBLK = 48
N_KV = 8


def key_field(key):
    drawn = jax.random.normal(jax.random.fold_in(key, 11), (SEQS, SEQ, KVH * HD), jnp.float32)
    return jnp.clip(drawn, -4.0, 4.0)


def draw_key_states(key, part):
    return key_field(key).astype(jnp.bfloat16)


def draw_queries(key, part):
    drawn = jnp.clip(jax.random.normal(jax.random.fold_in(key, 23), (SEQS, SEQ, H * HD), jnp.float32), -4.0, 4.0)
    return drawn.astype(jnp.bfloat16)


def draw_chosen(key, part):
    blocks = jnp.arange(NBLK, dtype=jnp.int32)
    holder = blocks // BPD
    within = blocks % BPD
    query_dev = blocks // BPD
    query_in = blocks % BPD
    jitter = jax.random.randint(jax.random.fold_in(key, 3), (SEQS, N_KV, KVH, NBLK), 0, 1024)
    ranking = jitter * BPD + within
    ranking = jnp.where(blocks == 0, 1024 * BPD + 1, ranking)
    grouped = ranking.reshape(SEQS, N_KV, KVH, N_KV, BPD)
    order_rank = jnp.sum((grouped[..., None, :] > grouped[..., :, None]).astype(jnp.int32), axis=-1)
    usable = (order_rank < MOST).reshape(SEQS, N_KV, KVH, NBLK)
    usable_q = usable[:, query_dev]
    earlier = (holder[None, :] < query_dev[:, None])[None, :, None, :]
    own_ok = (holder[None, :] == query_dev[:, None]) & (within[None, :] <= query_in[:, None])
    forced = (own_ok | (blocks == 0)[None, :])[None, :, None, :]
    future = (blocks[None, :] > blocks[:, None])[None, :, None, :]
    levels = jnp.where(forced, 3, jnp.where(earlier & usable_q, 2, jnp.where(future, 1, 0)))
    pick_noise = jax.random.randint(jax.random.fold_in(key, 5), (SEQS, NBLK, KVH, NBLK), 0, 512)
    distance = query_dev[:, None] - holder[None, :]
    closeness = jnp.clip(512 - 64 * distance, 0, 1023)
    skewed = pick_noise + closeness[None, :, None, :]
    nearness = 1023 - jnp.minimum(jnp.abs(blocks[None, :] - blocks[:, None]), 1023)
    secondary = jnp.where(levels == 1, nearness[None, :, None, :], skewed)
    priority = levels * 2 ** 22 + secondary * NBLK + blocks[None, None, None, :]
    values_top, picked = lax.top_k(priority.astype(jnp.int32), TOPK)
    return picked.astype(jnp.int32)


def level_of(own_key, shape, shards, smallest, top_value):
    loudness = 1.0
    for axis_at, shards_of in shards:
        heights = jax.random.uniform(jax.random.fold_in(jax.random.fold_in(own_key, 6), axis_at), (shards_of,), jnp.float32, smallest / len(shards), top_value / len(shards))
        loudness = loudness * jnp.repeat(jnp.exp(heights), shape[axis_at] // shards_of).reshape((-1,) + (1,) * (len(shape) - 1 - axis_at))
    return loudness


def centred(key, shape, deviation, bound, shards=(), held_as=jnp.bfloat16):
    result = jax.random.normal(key, shape, jnp.float32) * deviation
    if len(shards) > 0:
        result = level_of(key, shape, shards, -0.22, 0.18) * result
    return jnp.clip(result, min=-bound, max=bound).astype(held_as)


def setup_inputs(seed: int = 0) -> dict:
    key_list = jax.random.split(jax.random.key(seed), 8)
    return {
        "queries": draw_queries(jax.random.fold_in(key_list[7], 71), 0),
        "key_states": draw_key_states(jax.random.fold_in(key_list[7], 71), 0),
        "value_states": centred(key_list[2], (SEQS, SEQ, KVH * HD), 1.0, 6.0, ((1, 8), (2, 4))),
        "cotangent": centred(key_list[3], (SEQS, SEQ, H * HD), 1.0, 6.0, ((1, 8), (2, 4))),
        "gate_logits": centred(key_list[4], (SEQS, SEQ, H), 1.5, 6.0, ((1, 8), (2, 4)), jnp.float32),
        "layer_input": centred(key_list[5], (SEQS, SEQ, D), 1.0, 6.0, ((1, 32),)),
        "chosen": draw_chosen(jax.random.fold_in(key_list[7], 71), 0),
    }


def reference(queries, key_states, value_states, cotangent, gate_logits, layer_input, chosen):
    seq_count, seq_len, row_width = queries.shape
    per_group = H // KVH
    total_blocks = seq_len // BLK
    score_scale = HD ** -0.5
    key_blocks = key_states.reshape(seq_count, total_blocks, BLK, KVH, HD)
    value_blocks = value_states.reshape(seq_count, total_blocks, BLK, KVH, HD)
    query_blocks = queries.reshape(seq_count, total_blocks, BLK, KVH, per_group, HD)
    grad_blocks = cotangent.reshape(seq_count, total_blocks, BLK, KVH, per_group, HD)
    gate_values = jax.nn.sigmoid(gate_logits.astype(jnp.float32)).reshape(seq_count, total_blocks, BLK, KVH, per_group)
    group_index = jnp.arange(KVH, dtype=jnp.int32)[:, None]
    offsets = jnp.arange(BLK, dtype=jnp.int32)

    def advance(totals, position):
        key_acc, value_acc = totals
        seq_index = position // total_blocks
        block_index = position % total_blocks
        picked = chosen[seq_index, block_index]
        picked_keys = key_blocks[seq_index][picked, :, group_index].astype(jnp.float32)
        picked_values = value_blocks[seq_index][picked, :, group_index].astype(jnp.float32)
        query_rows = query_blocks[seq_index, block_index].astype(jnp.float32)
        scores = jnp.einsum("qgpd,gknd->gpqkn", query_rows, picked_keys) * score_scale
        query_pos = block_index * BLK + offsets
        key_pos = picked[:, :, None] * BLK + offsets
        allowed = key_pos[:, None, None, :, :] <= query_pos[None, None, :, None, None]
        scores = jnp.where(allowed, scores, -jnp.inf)
        row_max = jnp.max(scores, axis=(3, 4), keepdims=True)
        exp_terms = jnp.exp(scores - row_max)
        weights = exp_terms / jnp.sum(exp_terms, axis=(3, 4), keepdims=True)
        weights_bf = weights.astype(jnp.bfloat16).astype(jnp.float32)
        branch_out = jnp.einsum("gpqkn,gknd->qgpd", weights_bf, picked_values)
        branch_grad = (gate_values[seq_index, block_index][..., None] * grad_blocks[seq_index, block_index].astype(jnp.float32)).astype(jnp.bfloat16).astype(jnp.float32)
        row_dot = jnp.sum(branch_grad * branch_out, axis=3)
        weight_grad = jnp.einsum("qgpd,gknd->gpqkn", branch_grad, picked_values)
        score_grad = (weights * (weight_grad - jnp.transpose(row_dot, (1, 2, 0))[..., None, None]) * score_scale).astype(jnp.bfloat16).astype(jnp.float32)
        query_grad = jnp.einsum("gpqkn,gknd->qgpd", score_grad, picked_keys).astype(jnp.bfloat16)
        pick_key = jnp.einsum("gpqkn,qgpd->gknd", score_grad, query_rows)
        pick_value = jnp.einsum("gpqkn,qgpd->gknd", weights_bf, branch_grad)
        key_acc = key_acc.at[seq_index, picked, :, group_index].add(pick_key)
        value_acc = value_acc.at[seq_index, picked, :, group_index].add(pick_value)
        return (key_acc, value_acc), query_grad

    empty = jnp.zeros((seq_count, total_blocks, BLK, KVH, HD), jnp.float32)
    (key_acc, value_acc), query_parts = lax.scan(advance, (empty, empty), jnp.arange(seq_count * total_blocks, dtype=jnp.int32))
    query_grad = query_parts.reshape(seq_count, seq_len, H * HD)
    key_grad = key_acc.reshape(seq_count, seq_len, KVH * HD).astype(jnp.bfloat16)
    value_grad = value_acc.reshape(seq_count, seq_len, KVH * HD).astype(jnp.bfloat16)
    value_weight_grad = jnp.einsum("std,ste->de", layer_input.astype(jnp.float32), value_grad.astype(jnp.float32))
    return query_grad, key_grad, value_grad, value_weight_grad
```

```python
import functools
import math

import jax
import jax.numpy as jnp
from jax import lax
from jax.experimental import pallas as pl
from jax.experimental.pallas import tpu as pltpu
from jax.sharding import PartitionSpec as P

BLK = 64
MOST = 2
NEG = -1e30
LANES = 128
MESH = pl.DeviceIdType.MESH


def greet(devs, tps, me, my_tp):
    barrier = pltpu.get_barrier_semaphore()

    def kv_peer(d, carry):
        pl.semaphore_signal(
            barrier, inc=1, device_id={"kv": lax.rem(me + d, devs)}, device_id_type=MESH
        )
        return carry

    lax.fori_loop(1, devs, kv_peer, 0)
    for d in range(1, tps):
        pl.semaphore_signal(
            barrier, inc=1, device_id={"tp": lax.rem(my_tp + d, tps)}, device_id_type=MESH
        )
    pl.semaphore_wait(barrier, devs - 1 + tps - 1)


def fetch(
    devs, tps, seqs, own, share, groups,
    hot_ref, near_ref, li_ref,
    far_ref, asked_ref, rows_ref,
    reply_ref, hot_send, hot_recv, far_send, far_recv, li_send, li_recv, li_sem,
):
    me = lax.axis_index("kv")
    my_tp = lax.axis_index("tp")
    greet(devs, tps, me, my_tp)
    pos = li_ref.shape[1]

    def ask(m, src):
        return pltpu.make_async_remote_copy(
            src_ref=hot_ref.at[m], dst_ref=asked_ref.at[src],
            send_sem=hot_send.at[m], recv_sem=hot_recv.at[src],
            device_id={"kv": m}, device_id_type=MESH,
        )

    def answer(n, src):
        return pltpu.make_async_remote_copy(
            src_ref=reply_ref.at[n], dst_ref=far_ref.at[src],
            send_sem=far_send.at[n], recv_sem=far_recv.at[src],
            device_id={"kv": n}, device_id_type=MESH,
        )

    def columns(g, t):
        at = g * tps + t if groups == devs else t * groups + g
        return pl.ds(pl.multiple_of(at * share, share), share)

    def shuffle(g, t, src):
        return pltpu.make_async_remote_copy(
            src_ref=li_ref.at[:, :, columns(g, t)],
            dst_ref=rows_ref.at[g, :, pl.ds(pl.multiple_of(src * pos, pos), pos), :],
            send_sem=li_send.at[t, g], recv_sem=li_recv.at[src, g],
            device_id={"tp": t}, device_id_type=MESH,
        )

    def keep(g):
        return pltpu.make_async_copy(
            li_ref.at[:, :, columns(g, my_tp)],
            rows_ref.at[g, :, pl.ds(pl.multiple_of(my_tp * pos, pos), pos), :],
            li_sem.at[g],
        )

    def loop(lo, hi, body):
        def step(i, carry):
            body(i)
            return carry

        lax.fori_loop(lo, hi, step, 0)

    loop(0, me, lambda m: ask(m, me).start())
    for d in range(1, tps):
        t = lax.rem(my_tp + d, tps)
        loop(0, groups, lambda g: shuffle(g, t, my_tp).start())
    loop(0, groups, lambda g: keep(g).start())

    def blank(m):
        far_ref[m] = jnp.zeros(far_ref.shape[1:], far_ref.dtype)

    loop(me, devs - 1, blank)

    def reply(i):
        n = devs - 1 - i
        ask(n, n).wait_recv()
        for s in range(seqs):
            for j in range(MOST):
                total = None
                for b in range(own):
                    row = asked_ref[n, s, j, b : b + 1, :]
                    term = row * near_ref[s, b * BLK : (b + 1) * BLK, :]
                    total = term if total is None else total + term
                reply_ref[n, s, j * BLK : (j + 1) * BLK, :] = total
        answer(n, me).start()

    loop(0, devs - 1 - me, reply)
    loop(0, me, lambda m: answer(m, m).wait_recv())
    for d in range(1, tps):
        t = lax.rem(my_tp + d, tps)
        loop(0, groups, lambda g: shuffle(g, t, t).wait_recv())
        loop(0, groups, lambda g: shuffle(g, t, my_tp).wait_send())
    loop(0, groups, lambda g: keep(g).wait())
    loop(0, me, lambda m: ask(m, me).wait_send())
    loop(me + 1, devs, lambda n: answer(n, me).wait_send())


def attend(
    heads, hd, slots, own,
    bias_ref, q_ref, c_ref, g_ref, far_ref, near_ref,
    dq_ref, out_ref, dnear_ref, kv_ref, dkv_ref,
):
    qb = pl.program_id(1)
    blk = q_ref.shape[1]
    far_rows = slots * blk

    @pl.when(qb == 0)
    def _():
        kv_ref[:far_rows] = far_ref[:, 0].reshape(far_rows, 2 * hd)
        kv_ref[far_rows:] = near_ref[0]

    scale = hd**-0.5
    q = q_ref[0]
    cot = c_ref[0].astype(jnp.float32)
    gate = jax.nn.sigmoid(g_ref[0])
    qs = jnp.concatenate([q[:, h * hd : (h + 1) * hd] for h in range(heads)], axis=0)
    bg = jnp.concatenate(
        [gate[:, h : h + 1] * cot[:, h * hd : (h + 1) * hd] for h in range(heads)], axis=0
    ).astype(jnp.bfloat16)
    keys = kv_ref[:, :hd]
    vals = kv_ref[:, hd:]
    dims = (((1,), (1,)), ((), ()))
    raw = lax.dot_general(keys, qs, dims, preferred_element_type=jnp.float32)
    raw = raw * (scale * math.log2(math.e))
    rows = heads * blk
    key_in = lax.broadcasted_iota(jnp.int32, (blk, rows), 0)
    row_in = lax.rem(lax.broadcasted_iota(jnp.int32, (blk, rows), 1), blk)
    ahead = key_in - row_in
    parts = []
    for c in range(slots + own):
        part = raw[c * blk : (c + 1) * blk] + bias_ref[pl.program_id(0), qb, c]
        if c >= slots:
            part = jnp.where(ahead <= (qb - (c - slots)) * blk, part, NEG)
        parts.append(part)
    s = jnp.concatenate(parts, axis=0)
    top = jnp.max(s, axis=0, keepdims=True)
    p = jnp.exp2(s - top)
    inv = 1.0 / jnp.sum(p, axis=0, keepdims=True)
    w = p * inv
    wb = w.astype(jnp.bfloat16)
    wg = lax.dot_general(vals, bg, dims, preferred_element_type=jnp.float32)
    dot = jnp.sum(wb.astype(jnp.float32) * wg, axis=0, keepdims=True)
    ds = (w * (wg - dot) * scale).astype(jnp.bfloat16)
    dqt = lax.dot_general(
        keys, ds, (((0,), (0,)), ((), ())), preferred_element_type=jnp.float32
    )
    dq = dqt.T
    dq_ref[0] = jnp.concatenate(
        [dq[h * blk : (h + 1) * blk] for h in range(heads)], axis=1
    ).astype(jnp.bfloat16)
    dk = jnp.dot(ds, qs, preferred_element_type=jnp.float32)
    dv = jnp.dot(wb, bg, preferred_element_type=jnp.float32)
    dkv = jnp.concatenate([dk, dv], axis=1)

    @pl.when(qb == 0)
    def _():
        dkv_ref[...] = dkv

    @pl.when(qb > 0)
    def _():
        dkv_ref[...] += dkv

    @pl.when(qb == own - 1)
    def _():
        out_ref[:, 0] = dkv_ref[:far_rows].astype(jnp.bfloat16).reshape(out_ref.shape[0], MOST * blk, 2 * hd)
        dnear_ref[0] = dkv_ref[far_rows:]


def combine(
    devs, tps, seqs, own, hd, groups,
    out_ref, dnear_ref, asked_ref, rows_ref,
    kg_ref, vgrad_ref, wg_ref,
    back_ref, total_ref, vg_ref, mat_ref, part_ref, piece_ref,
    back_send, back_recv, vg_send, vg_recv, piece_send, piece_recv,
):
    me = lax.axis_index("kv")
    my_tp = lax.axis_index("tp")
    greet(devs, tps, me, my_tp)
    toks = own * BLK

    def back(m, src):
        return pltpu.make_async_remote_copy(
            src_ref=out_ref.at[m], dst_ref=back_ref.at[src],
            send_sem=back_send.at[m], recv_sem=back_recv.at[src],
            device_id={"kv": m}, device_id_type=MESH,
        )

    def spread(t, src):
        return pltpu.make_async_remote_copy(
            src_ref=vg_ref.at[src], dst_ref=vg_ref.at[src],
            send_sem=vg_send.at[t], recv_sem=vg_recv.at[src],
            device_id={"tp": t}, device_id_type=MESH,
        )

    def piece(kv, src):
        return pltpu.make_async_remote_copy(
            src_ref=part_ref.at[kv], dst_ref=piece_ref.at[src],
            send_sem=piece_send.at[kv], recv_sem=piece_recv.at[src],
            device_id={"kv": kv}, device_id_type=MESH,
        )

    def loop(lo, hi, body):
        def step(i, carry):
            body(i)
            return carry

        lax.fori_loop(lo, hi, step, 0)

    loop(0, me, lambda m: back(m, me).start())
    total_ref[...] = dnear_ref[...]

    def add(n):
        back(0, n).wait_recv()
        for s in range(seqs):
            for b in range(own):
                term = None
                for j in range(MOST):
                    row = asked_ref[n, s, j, b : b + 1, :].astype(jnp.float32)
                    more = row * back_ref[n, s, j * BLK : (j + 1) * BLK, :].astype(jnp.float32)
                    term = more if term is None else term + more
                total_ref[s, b * BLK : (b + 1) * BLK, :] += term

    loop(me + 1, devs, add)
    both = total_ref[...].astype(jnp.bfloat16)
    kg_ref[...] = both[:, :, :hd]
    vgrad_ref[...] = both[:, :, hd:]
    for s in range(seqs):
        vg_ref[my_tp, :, s * hd : (s + 1) * hd] = both[s, :, hd:]
    for d in range(1, tps):
        spread(lax.rem(my_tp + d, tps), my_tp).start()
    for d in range(1, tps):
        t = lax.rem(my_tp + d, tps)
        spread(t, t).wait_recv()
    for t in range(tps):
        for s in range(seqs):
            mat_ref[s * toks : (s + 1) * toks, t * hd : (t + 1) * hd] = vg_ref[t, :, s * hd : (s + 1) * hd]
    turned = mat_ref[...].T

    def product(g):
        rows = rows_ref[g].reshape(seqs * toks, rows_ref.shape[3])
        return jnp.dot(turned, rows, preferred_element_type=jnp.float32)

    if groups == devs:

        def stage(i):
            kv = lax.rem(me + 1 + i, devs)
            part_ref[kv] = product(kv).astype(jnp.bfloat16)

            @pl.when(i < devs - 1)
            def _():
                piece(kv, me).start()

        loop(0, devs, stage)
    else:

        def stage(g):
            part_ref[pl.ds(g * (devs // groups), devs // groups)] = (
                product(g).T.astype(jnp.bfloat16).reshape((devs // groups,) + part_ref.shape[1:])
            )

        loop(0, groups, stage)
        loop(0, devs - 1, lambda i: piece(lax.rem(me + 1 + i, devs), me).start())
    piece_ref[me] = part_ref[me]

    def wait(i):
        n = lax.rem(me + 1 + i, devs)
        piece(n, n).wait_recv()

    loop(0, devs - 1, wait)
    result = piece_ref[0].astype(jnp.float32)
    for n in range(1, devs):
        result += piece_ref[n].astype(jnp.float32)
    wg_ref[...] = result.T if groups == devs else result
    loop(0, me, lambda m: back(m, me).wait_send())
    for d in range(1, tps):
        spread(lax.rem(my_tp + d, tps), my_tp).wait_send()

    def sent(i):
        piece(lax.rem(me + 1 + i, devs), me).wait_send()

    loop(0, devs - 1, sent)


def on_device(queries, key_states, value_states, cotangent, gate_logits, layer_input, chosen):
    seqs, toks, width = queries.shape
    hd = key_states.shape[2]
    heads = width // hd
    own = toks // BLK
    devs = lax.axis_size("kv")
    tps = lax.axis_size("tp")
    me = lax.axis_index("kv")
    total = devs * own
    pos = layer_input.shape[1]
    share = layer_input.shape[2] // (devs * tps)

    ids = chosen[:, :, 0, :]
    blocks = jnp.arange(total, dtype=jnp.int32)
    named = jnp.any(ids[..., None] == blocks, axis=2)
    seen = jnp.any(named, axis=1) & (blocks // own < me)
    seen = seen.reshape(seqs, devs, own)
    inner = jnp.arange(own, dtype=jnp.int32)
    before = jnp.sum(
        (seen[:, :, None, :] & (inner[None, :] < inner[:, None])).astype(jnp.int32), axis=3
    )
    slot = (before[:, :, None, :] == jnp.arange(MOST, dtype=jnp.int32)[:, None]) & seen[:, :, None, :]
    pad = -own % 8
    hot = jnp.pad(jnp.transpose(slot, (1, 0, 2, 3)), ((0, 0), (0, 0), (0, 0), (0, pad)))
    hot = jnp.broadcast_to(hot[..., None], hot.shape + (LANES,)).astype(jnp.bfloat16)

    by_dev = named.reshape(seqs, own, devs, own)
    far_ok = jnp.any(by_dev[:, :, :, None, :] & slot[:, None], axis=4)[:, :, : devs - 1]
    slots = (devs - 1) * MOST
    far_ok = far_ok.reshape(seqs, own, slots)
    near_ok = jnp.any(by_dev & (jnp.arange(devs, dtype=jnp.int32) == me)[:, None], axis=2)
    ok = jnp.concatenate([far_ok, near_ok], axis=2)
    bias = jnp.where(ok, 0.0, NEG).astype(jnp.float32)

    groups, cut = devs, share
    if share % LANES:
        groups, cut = devs * share // LANES, LANES
        layer_input = layer_input.reshape(seqs, pos, devs, tps, share)
        layer_input = jnp.swapaxes(layer_input, 2, 3).reshape(seqs, pos, devs * tps * share)
    part = (tps * hd, share) if groups == devs else (share, tps * hd)

    near = jnp.concatenate([key_states, value_states], axis=-1)
    vmem = pl.BlockSpec(memory_space=pltpu.VMEM)
    hbm = pl.BlockSpec(memory_space=pl.ANY)
    blocks_of = (seqs, MOST * BLK, 2 * hd)
    far, asked, rows = pl.pallas_call(
        functools.partial(fetch, devs, tps, seqs, own, cut, groups),
        in_specs=[vmem, vmem, hbm],
        out_specs=[vmem, vmem, vmem],
        out_shape=[
            jax.ShapeDtypeStruct((devs - 1,) + blocks_of, jnp.bfloat16),
            jax.ShapeDtypeStruct(hot.shape, jnp.bfloat16),
            jax.ShapeDtypeStruct((groups, seqs, toks, cut), jnp.bfloat16),
        ],
        scratch_shapes=[
            pltpu.VMEM((devs,) + blocks_of, jnp.bfloat16),
            pltpu.SemaphoreType.DMA((devs,)),
            pltpu.SemaphoreType.DMA((devs,)),
            pltpu.SemaphoreType.DMA((devs,)),
            pltpu.SemaphoreType.DMA((devs,)),
            pltpu.SemaphoreType.DMA((tps, groups)),
            pltpu.SemaphoreType.DMA((tps, groups)),
            pltpu.SemaphoreType.DMA((groups,)),
        ],
        compiler_params=pltpu.CompilerParams(
            collective_id=0, has_side_effects=True, vmem_limit_bytes=24 * 2**20
        ),
    )(hot, near, layer_input)

    keys = (slots + own) * BLK
    pairs = seqs * own * heads * BLK * keys
    query_grad, out, dnear = pl.pallas_call(
        functools.partial(attend, heads, hd, slots, own),
        grid=(seqs, own),
        in_specs=[
            pl.BlockSpec(memory_space=pltpu.SMEM),
            pl.BlockSpec((1, BLK, width), lambda s, b: (s, b, 0)),
            pl.BlockSpec((1, BLK, width), lambda s, b: (s, b, 0)),
            pl.BlockSpec((1, BLK, heads), lambda s, b: (s, b, 0)),
            pl.BlockSpec((devs - 1, 1, MOST * BLK, 2 * hd), lambda s, b: (0, s, 0, 0)),
            pl.BlockSpec((1, toks, 2 * hd), lambda s, b: (s, 0, 0)),
        ],
        out_specs=[
            pl.BlockSpec((1, BLK, width), lambda s, b: (s, b, 0)),
            pl.BlockSpec((devs - 1, 1, MOST * BLK, 2 * hd), lambda s, b: (0, s, 0, 0)),
            pl.BlockSpec((1, toks, 2 * hd), lambda s, b: (s, 0, 0)),
        ],
        out_shape=[
            jax.ShapeDtypeStruct((seqs, toks, width), jnp.bfloat16),
            jax.ShapeDtypeStruct((devs - 1,) + blocks_of, jnp.bfloat16),
            jax.ShapeDtypeStruct((seqs, toks, 2 * hd), jnp.float32),
        ],
        scratch_shapes=[
            pltpu.VMEM((keys, 2 * hd), jnp.bfloat16),
            pltpu.VMEM((keys, 2 * hd), jnp.float32),
        ],
        cost_estimate=pl.CostEstimate(
            flops=pairs * hd * 20, bytes_accessed=8 * 2**20, transcendentals=pairs
        ),
        compiler_params=pltpu.CompilerParams(
            dimension_semantics=("arbitrary", "arbitrary"), vmem_limit_bytes=48 * 2**20
        ),
    )(bias, queries, cotangent, gate_logits, far, near)

    return (query_grad,) + tuple(
        pl.pallas_call(
            functools.partial(combine, devs, tps, seqs, own, hd, groups),
            in_specs=[vmem] * 4,
            out_specs=[vmem] * 3,
            out_shape=[
                jax.ShapeDtypeStruct((seqs, toks, hd), jnp.bfloat16),
                jax.ShapeDtypeStruct((seqs, toks, hd), jnp.bfloat16),
                jax.ShapeDtypeStruct((share, tps * hd), jnp.float32),
            ],
            scratch_shapes=[
                pltpu.VMEM((devs,) + blocks_of, jnp.bfloat16),
                pltpu.VMEM((seqs, toks, 2 * hd), jnp.float32),
                pltpu.VMEM((tps, toks, seqs * hd), jnp.bfloat16),
                pltpu.VMEM((seqs * toks, tps * hd), jnp.bfloat16),
                pltpu.VMEM((devs,) + part, jnp.bfloat16),
                pltpu.VMEM((devs,) + part, jnp.bfloat16),
                pltpu.SemaphoreType.DMA((devs,)),
                pltpu.SemaphoreType.DMA((devs,)),
                pltpu.SemaphoreType.DMA((tps,)),
                pltpu.SemaphoreType.DMA((tps,)),
                pltpu.SemaphoreType.DMA((devs,)),
                pltpu.SemaphoreType.DMA((devs,)),
            ],
            compiler_params=pltpu.CompilerParams(
                collective_id=1, has_side_effects=True, vmem_limit_bytes=32 * 2**20
            ),
        )(out, dnear, asked, rows)
    )


def solution(mesh):
    in_specs = (
        P(None, "kv", "tp"),
        P(None, "kv", "tp"),
        P(None, "kv", "tp"),
        P(None, "kv", "tp"),
        P(None, "kv", "tp"),
        P(None, ("kv", "tp"), None),
        P(None, "kv", "tp", None),
    )
    out_specs = (
        P(None, "kv", "tp"),
        P(None, "kv", "tp"),
        P(None, "kv", "tp"),
        P(("kv", "tp"), None),
    )
    return jax.shard_map(
        on_device, mesh=mesh, in_specs=in_specs, out_specs=out_specs, check_vma=False
    )
```

```python
import functools
import math

import jax
import jax.numpy as jnp
from jax import lax
from jax.experimental import pallas as pl
from jax.experimental.pallas import tpu as pltpu
from jax.sharding import PartitionSpec as P

BLK = 64
MOST = 2
PAIR = 2
SUB = 8
LANES = 128
NEG = -1e30
MESH = pl.DeviceIdType.MESH
BF = jnp.bfloat16
F32 = jnp.float32


def loop(lo, hi, body):
    def step(i, carry):
        body(i)
        return carry

    lax.fori_loop(lo, hi, step, 0)


def fold(count, body, carry):
    if count <= 8:
        for i in range(count):
            carry = body(i, carry)
        return carry
    return lax.fori_loop(0, count, body, carry)


def at(i, size):
    return pl.ds(i * size, size) if isinstance(i, int) else pl.ds(pl.multiple_of(i * size, size), size)


def whole(
    devs, tps, seqs, own, heads, hd, share, groups,
    chosen_ref, q_ref, c_ref, g_ref, k_ref, v_ref, li_ref,
    dq_ref, kg_ref, vo_ref, wg_ref,
    near_ref, gate_ref, named_ref, hot_ref, asked_ref, farb_ref, nearb_ref,
    reply_ref, far_ref, rows_ref, kt_ref, s_ref, w_ref, ds_ref, dkv_ref,
    out_ref, total_ref, back_ref, vg_ref, acc_ref, part_ref, piece_ref,
    hot_send, hot_recv, far_send, far_recv, li_send, li_recv, li_sem,
    back_send, back_recv, vg_send, vg_recv, piece_send, piece_recv,
):
    me = lax.axis_index("kv")
    my_tp = lax.axis_index("tp")
    toks = own * BLK
    pos = li_ref.shape[1]
    pairs = own // PAIR
    wide = PAIR * BLK
    far_rows = MOST * BLK
    scale = hd**-0.5
    log2e = math.log2(math.e)

    barrier = pltpu.get_barrier_semaphore()
    loop(1, devs, lambda d: pl.semaphore_signal(
        barrier, inc=1, device_id={"kv": lax.rem(me + d, devs)}, device_id_type=MESH
    ))
    for d in range(1, tps):
        pl.semaphore_signal(
            barrier, inc=1, device_id={"tp": lax.rem(my_tp + d, tps)}, device_id_type=MESH
        )

    def ask(m, src):
        return pltpu.make_async_remote_copy(
            src_ref=hot_ref.at[m], dst_ref=asked_ref.at[src],
            send_sem=hot_send.at[m], recv_sem=hot_recv.at[src],
            device_id={"kv": m}, device_id_type=MESH,
        )

    def answer(s, n, src):
        return pltpu.make_async_remote_copy(
            src_ref=reply_ref.at[s, n], dst_ref=far_ref.at[s, src],
            send_sem=far_send.at[s, n], recv_sem=far_recv.at[s, src],
            device_id={"kv": n}, device_id_type=MESH,
        )

    def columns(g, t):
        return at(g * tps + t if groups == devs else t * groups + g, share)

    def shuffle(g, t, src):
        return pltpu.make_async_remote_copy(
            src_ref=li_ref.at[:, :, columns(g, t)],
            dst_ref=rows_ref.at[g, :, at(src, pos), :],
            send_sem=li_send.at[t, g], recv_sem=li_recv.at[src, g],
            device_id={"tp": t}, device_id_type=MESH,
        )

    def keep(g):
        return pltpu.make_async_copy(
            li_ref.at[:, :, columns(g, my_tp)], rows_ref.at[g, :, at(my_tp, pos), :], li_sem.at[g]
        )

    def back(s, m, src):
        return pltpu.make_async_remote_copy(
            src_ref=out_ref.at[s, m], dst_ref=back_ref.at[s, src],
            send_sem=back_send.at[s, m], recv_sem=back_recv.at[s, src],
            device_id={"kv": m}, device_id_type=MESH,
        )

    def spread(s, t, src):
        return pltpu.make_async_remote_copy(
            src_ref=vg_ref.at[s, at(src, hd), :], dst_ref=vg_ref.at[s, at(src, hd), :],
            send_sem=vg_send.at[s, t], recv_sem=vg_recv.at[s, src],
            device_id={"tp": t}, device_id_type=MESH,
        )

    def piece(kv, src):
        return pltpu.make_async_remote_copy(
            src_ref=part_ref.at[kv], dst_ref=piece_ref.at[src],
            send_sem=piece_send.at[kv], recv_sem=piece_recv.at[src],
            device_id={"kv": kv}, device_id_type=MESH,
        )

    peers = [lax.rem(my_tp + d, tps) for d in range(1, tps)]

    count = devs * SUB
    row = lax.broadcasted_iota(jnp.int32, (count, LANES), 0)
    lane = lax.broadcasted_iota(jnp.int32, (devs, LANES), 1)
    holder, inner = row // SUB, row % SUB
    block = jnp.where(inner < own, holder * own + inner, -1)
    topk = chosen_ref.shape[3]
    across = lax.broadcasted_iota(jnp.int32, (count, count), 1)
    down = lax.broadcasted_iota(jnp.int32, (count, count), 0)
    lower = jnp.where((across // SUB == down // SUB) & (across < down), 1.0, 0.0).astype(BF)
    for s in range(seqs):
        seen = jnp.zeros((count, LANES), F32)
        named = []
        for b in range(own):
            hit = jnp.where(block[:, :topk] == chosen_ref[s, b], 1.0, 0.0)
            hit = jnp.broadcast_to(jnp.max(hit, axis=1, keepdims=True), (count, LANES))
            named_ref[s * own + b] = hit.reshape(devs, SUB, LANES)
            named.append(hit)
            seen = jnp.maximum(seen, hit)
        seen = jnp.where(holder < me, seen, 0.0)
        rank = jnp.dot(lower, seen.astype(BF), preferred_element_type=F32)
        for j in range(MOST):
            hot = jnp.where(rank == j, seen, 0.0)
            hot_ref[:, s, j] = hot.reshape(devs, SUB, LANES)
            oks = [jnp.sum((hot * n).reshape(devs, SUB, LANES), axis=1) for n in named]
            for t in range(pairs):
                ok = jnp.where(lane < BLK, oks[PAIR * t], oks[PAIR * t + 1])
                farb_ref[s * pairs + t, j] = (1.0 - ok) * NEG
        for t in range(pairs):
            ok = jnp.where(
                lane[:SUB] < BLK,
                named_ref[s * own + PAIR * t, me],
                named_ref[s * own + PAIR * t + 1, me],
            )
            nearb_ref[s * pairs + t] = (1.0 - ok) * NEG

    pl.semaphore_wait(barrier, devs - 1 + tps - 1)
    loop(0, me, lambda m: ask(m, me).start())
    for t in peers:
        loop(0, groups, lambda g: shuffle(g, t, my_tp).start())
    loop(0, groups, lambda g: keep(g).start())

    for s in range(seqs):
        near_ref[s] = jnp.concatenate([k_ref[s], v_ref[s]], axis=0).T
        gate_ref[s] = jax.nn.sigmoid(g_ref[s]).T

    def blank(m):
        for s in range(seqs):
            far_ref[s, m] = jnp.zeros(far_ref.shape[2:], BF)

    loop(me, devs - 1, blank)

    for s in range(seqs):

        def reply(i):
            n = devs - 1 - i
            if s == 0:
                ask(0, n).wait_recv()
            for j in range(MOST):
                total = None
                for b in range(own):
                    one = asked_ref[n, s, j, b : b + 1, :].astype(BF)
                    term = one * near_ref[s, b * BLK : (b + 1) * BLK, :]
                    total = term if total is None else total + term
                reply_ref[s, n, j * BLK : (j + 1) * BLK, :] = total
            answer(s, n, me).start()

        loop(0, devs - 1 - me, reply)

    chunks = devs - 1
    rows = heads * wide

    def attention(s):
        loop(0, me, lambda m: answer(s, 0, m).wait_recv())

        def turn(m, carry):
            kt_ref[:, at(m, far_rows)] = (far_ref[s, m][:, :hd] * scale).astype(BF).T
            return carry

        fold(chunks, turn, 0)
        for c in range(pairs):
            kt_ref[:, chunks * far_rows + c * wide : chunks * far_rows + (c + 1) * wide] = (
                (near_ref[s, c * wide : (c + 1) * wide, :hd] * scale).astype(BF).T
            )

        for t in range(pairs):
            tok = slice(t * wide, (t + 1) * wide)
            q = (q_ref[s, tok, :].astype(F32) * scale).astype(BF)
            cot = c_ref[s, tok, :].astype(F32)
            gate = gate_ref[s, tok, :]
            zero = jnp.zeros((rows, hd), BF)
            qs = jnp.concatenate([q[:, h * hd : (h + 1) * hd] for h in range(heads)], axis=0)
            bg = jnp.concatenate(
                [gate[:, h : h + 1] * cot[:, h * hd : (h + 1) * hd] for h in range(heads)], axis=0
            ).astype(BF)
            qs = jnp.concatenate([qs, zero], axis=1)
            bg = jnp.concatenate([zero, bg], axis=1)
            dims = (((1,), (1,)), ((), ()))
            ahead = lax.broadcasted_iota(jnp.int32, (wide, rows), 0) <= lax.rem(
                lax.broadcasted_iota(jnp.int32, (wide, rows), 1), wide
            )
            st = s * pairs + t

            def load(kind, c):
                return far_ref[s, c] if kind else near_ref[s, c * wide : (c + 1) * wide, :]

            def place(kind, c):
                return at(c, far_rows) if kind else slice(
                    chunks * far_rows + c * wide, chunks * far_rows + (c + 1) * wide
                )

            def score(kind, c, top):
                kv = load(kind, c)
                raw = lax.dot_general(kv, qs, dims, preferred_element_type=F32) * log2e
                w_ref[place(kind, c), :] = lax.dot_general(kv, bg, dims, preferred_element_type=F32)
                halves = []
                for j in range(MOST if kind else PAIR):
                    if kind:
                        bias = farb_ref[st, j, pl.ds(c, 1), :]
                    else:
                        bias = nearb_ref[st, c * PAIR + j : c * PAIR + j + 1, :]
                    bias = jnp.concatenate([bias] * heads, axis=1)
                    halves.append(raw[j * BLK : (j + 1) * BLK] + bias)
                sc = jnp.concatenate(halves, axis=0)
                if not kind and c == t:
                    sc = jnp.where(ahead, sc, NEG)
                s_ref[place(kind, c), :] = sc
                return jnp.maximum(top, jnp.max(sc.reshape(-1, SUB, rows), axis=0))

            top = jnp.full((SUB, rows), NEG, F32)
            for c in range(t + 1):
                top = score(False, c, top)
            top = fold(chunks, functools.partial(score, True), top)
            top = jnp.max(top, axis=0, keepdims=True)

            def weigh(kind, c, carry):
                norm, dot = carry
                p = jnp.exp2(s_ref[place(kind, c), :] - top)
                s_ref[place(kind, c), :] = p
                norm += jnp.sum(p.reshape(-1, SUB, rows), axis=0)
                dot += jnp.sum((p * w_ref[place(kind, c), :]).reshape(-1, SUB, rows), axis=0)
                return norm, dot

            carry = (jnp.zeros((SUB, rows), F32), jnp.zeros((SUB, rows), F32))
            for c in range(t + 1):
                carry = weigh(False, c, carry)
            norm, dot = fold(chunks, functools.partial(weigh, True), carry)
            inv = 1.0 / jnp.sum(norm, axis=0, keepdims=True)
            dot = jnp.sum(dot, axis=0, keepdims=True) * inv

            def grad(kind, c, carry):
                w = s_ref[place(kind, c), :] * inv
                ds = (w * (w_ref[place(kind, c), :] - dot)).astype(BF)
                ds_ref[place(kind, c), :] = ds
                more = jnp.dot(ds, qs, preferred_element_type=F32)
                more += jnp.dot(w.astype(BF), bg, preferred_element_type=F32)
                if t == 0 or (not kind and c == t):
                    dkv_ref[place(kind, c), :] = more
                else:
                    dkv_ref[place(kind, c), :] += more
                return carry

            for c in range(t + 1):
                grad(False, c, 0)
            fold(chunks, functools.partial(grad, True), 0)
            used = chunks * far_rows + (t + 1) * wide
            dqt = jnp.dot(kt_ref[:, :used], ds_ref[:used, :], preferred_element_type=F32)
            dqt = jnp.concatenate([dqt[:, h * wide : (h + 1) * wide] for h in range(heads)], axis=0)
            dq_ref[s, tok, :] = dqt.T.astype(BF)

        def give(m):
            out_ref[s, m] = dkv_ref[at(m, far_rows), :].astype(BF)
            back(s, m, me).start()

        loop(0, me, give)
        total_ref[s] = dkv_ref[chunks * far_rows :, :]

    loop(0, seqs, attention)

    def product(s, g):
        return jnp.dot(vg_ref[s], rows_ref[g, s], preferred_element_type=F32)

    for t in peers:
        loop(0, groups, lambda g: shuffle(g, t, t).wait_recv())
    loop(0, groups, lambda g: keep(g).wait())
    for s in range(seqs):

        def add(n):
            back(s, 0, n).wait_recv()
            for b in range(own):
                term = None
                for j in range(MOST):
                    one = asked_ref[n, s, j, b : b + 1, :]
                    more = one * back_ref[s, n, j * BLK : (j + 1) * BLK, :].astype(F32)
                    term = more if term is None else term + more
                total_ref[s, b * BLK : (b + 1) * BLK, :] += term

        loop(me + 1, devs, add)
        both = total_ref[s].T.astype(BF)
        kg_ref[s] = both[:hd]
        vo_ref[s] = both[hd:]
        vg_ref[s, at(my_tp, hd), :] = both[hd:]
        for t in peers:
            spread(s, t, my_tp).start()
        if s < seqs - 1:
            for t in peers:
                spread(s, t, t).wait_recv()

            def early(g):
                if s == 0:
                    acc_ref[g] = product(s, g)
                else:
                    acc_ref[g] += product(s, g)

            loop(0, groups, early)

    for t in peers:
        spread(seqs - 1, t, t).wait_recv()

    def final(g):
        last = product(seqs - 1, g)
        return last if seqs == 1 else last + acc_ref[g]

    if groups == devs:

        def stage(i):
            kv = lax.rem(me + 1 + i, devs)
            part_ref[kv] = final(kv).astype(BF)

            @pl.when(i < devs - 1)
            def _():
                piece(kv, me).start()

        loop(0, devs, stage)
    else:
        each = devs // groups

        def stage(g):
            part_ref[pl.ds(g * each, each)] = final(g).T.astype(BF).reshape((each,) + part_ref.shape[1:])

        loop(0, groups, stage)
        loop(0, devs - 1, lambda i: piece(lax.rem(me + 1 + i, devs), me).start())
    piece_ref[me] = part_ref[me]

    def arrive(i):
        piece(0, lax.rem(me + 1 + i, devs)).wait_recv()

    loop(0, devs - 1, arrive)
    result = piece_ref[0].astype(F32)
    for n in range(1, devs):
        result += piece_ref[n].astype(F32)
    wg_ref[...] = result.T if groups == devs else result

    loop(0, me, lambda m: ask(m, me).wait_send())
    for t in peers:
        loop(0, groups, lambda g: shuffle(g, t, my_tp).wait_send())
    for s in range(seqs):
        loop(me + 1, devs, lambda n: answer(s, n, me).wait_send())
        loop(0, me, lambda m: back(s, m, me).wait_send())
        for t in peers:
            spread(s, t, my_tp).wait_send()
    loop(0, devs - 1, lambda i: piece(lax.rem(me + 1 + i, devs), me).wait_send())


def on_device(queries, key_states, value_states, cotangent, gate_logits, layer_input, chosen):
    seqs, toks, width = queries.shape
    hd = key_states.shape[2]
    heads = width // hd
    own = toks // BLK
    pairs = own // PAIR
    devs = lax.axis_size("kv")
    tps = lax.axis_size("tp")
    pos = layer_input.shape[1]
    share = layer_input.shape[2] // (devs * tps)
    groups, cut = devs, share
    if share % LANES:
        groups, cut = devs * share // LANES, LANES
        layer_input = layer_input.reshape(seqs, pos, devs, tps, share)
        layer_input = jnp.swapaxes(layer_input, 2, 3).reshape(seqs, pos, devs * tps * share)
    part = (tps * hd, share) if groups == devs else (share, tps * hd)
    keys = (devs - 1) * MOST * BLK + toks
    rows = heads * PAIR * BLK
    sent = (MOST * BLK, 2 * hd)

    vmem = pl.BlockSpec(memory_space=pltpu.VMEM)
    hbm = pl.BlockSpec(memory_space=pl.ANY)
    dma = pltpu.SemaphoreType.DMA
    query_grad, key_grad, value_grad, weight_grad = pl.pallas_call(
        functools.partial(whole, devs, tps, seqs, own, heads, hd, cut, groups),
        in_specs=[vmem] * 6 + [hbm],
        out_specs=[vmem] * 4,
        out_shape=[
            jax.ShapeDtypeStruct((seqs, toks, width), BF),
            jax.ShapeDtypeStruct((seqs, hd, toks), BF),
            jax.ShapeDtypeStruct((seqs, hd, toks), BF),
            jax.ShapeDtypeStruct((share, tps * hd), F32),
        ],
        scratch_shapes=[
            pltpu.VMEM((seqs, toks, 2 * hd), BF),
            pltpu.VMEM((seqs, toks, heads), F32),
            pltpu.VMEM((seqs * own, devs, SUB, LANES), F32),
            pltpu.VMEM((devs, seqs, MOST, SUB, LANES), F32),
            pltpu.VMEM((devs, seqs, MOST, SUB, LANES), F32),
            pltpu.VMEM((seqs * pairs, MOST, devs, LANES), F32),
            pltpu.VMEM((seqs * pairs, SUB, LANES), F32),
            pltpu.VMEM((seqs, devs) + sent, BF),
            pltpu.VMEM((seqs, devs - 1) + sent, BF),
            pltpu.VMEM((groups, seqs, toks, cut), BF),
            pltpu.VMEM((hd, keys), BF),
            pltpu.VMEM((keys, rows), F32),
            pltpu.VMEM((keys, rows), F32),
            pltpu.VMEM((keys, rows), BF),
            pltpu.VMEM((keys, 2 * hd), F32),
            pltpu.VMEM((seqs, devs - 1) + sent, BF),
            pltpu.VMEM((seqs, toks, 2 * hd), F32),
            pltpu.VMEM((seqs, devs) + sent, BF),
            pltpu.VMEM((seqs, tps * hd, toks), BF),
            pltpu.VMEM((groups, tps * hd, cut), F32),
            pltpu.VMEM((devs,) + part, BF),
            pltpu.VMEM((devs,) + part, BF),
            dma((devs,)), dma((devs,)),
            dma((seqs, devs)), dma((seqs, devs)),
            dma((tps, groups)), dma((tps, groups)), dma((groups,)),
            dma((seqs, devs)), dma((seqs, devs)),
            dma((seqs, tps)), dma((seqs, tps)),
            dma((devs,)), dma((devs,)),
        ],
        compiler_params=pltpu.CompilerParams(
            collective_id=0, has_side_effects=True, vmem_limit_bytes=56 * 2**20
        ),
    )(
        chosen, queries, cotangent, jnp.swapaxes(gate_logits, 1, 2),
        jnp.swapaxes(key_states, 1, 2), jnp.swapaxes(value_states, 1, 2), layer_input,
    )
    return query_grad, jnp.swapaxes(key_grad, 1, 2), jnp.swapaxes(value_grad, 1, 2), weight_grad


def solution(mesh):
    in_specs = (
        P(None, "kv", "tp"),
        P(None, "kv", "tp"),
        P(None, "kv", "tp"),
        P(None, "kv", "tp"),
        P(None, "kv", "tp"),
        P(None, ("kv", "tp"), None),
        P(None, "kv", "tp", None),
    )
    out_specs = (
        P(None, "kv", "tp"),
        P(None, "kv", "tp"),
        P(None, "kv", "tp"),
        P(("kv", "tp"), None),
    )
    return jax.shard_map(
        on_device, mesh=mesh, in_specs=in_specs, out_specs=out_specs, check_vma=False
    )
```

```python
import functools
import math

import jax
import jax.numpy as jnp
from jax import lax
from jax.experimental import pallas as pl
from jax.experimental.pallas import tpu as pltpu
from jax.sharding import PartitionSpec as P

BLK = 64
MOST = 2
PAIR = 2
SUB = 8
LANES = 128
NEG = -1e30
MESH = pl.DeviceIdType.MESH
BF = jnp.bfloat16
F32 = jnp.float32


def loop(lo, hi, body):
    def step(i, carry):
        body(i)
        return carry

    lax.fori_loop(lo, hi, step, 0)


def fold(count, body, carry):
    if count <= 8:
        for i in range(count):
            carry = body(i, carry)
        return carry
    return lax.fori_loop(0, count, body, carry)


def at(i, size):
    return pl.ds(i * size, size) if isinstance(i, int) else pl.ds(pl.multiple_of(i * size, size), size)


def whole(
    devs, tps, seqs, own, heads, hd, share, groups,
    chosen_ref, q_in, c_in, g_in, k_in, v_in, li_ref,
    dq_out, kg_out, vo_out, wg_out,
    q_ref, c_ref, g_ref, k_ref, v_ref, dq_ref, kg_ref, vo_ref, wg_ref,
    near_ref, gate_ref, named_ref, hot_ref, asked_ref, farb_ref, nearb_ref,
    reply_ref, far_ref, rows_ref, kt_ref, s_ref, w_ref, ds_ref, dkv_ref,
    out_ref, total_ref, back_ref, vg_ref, acc_ref, part_ref, piece_ref,
    hot_send, hot_recv, far_send, far_recv, li_send, li_recv, li_sem,
    back_send, back_recv, vg_send, vg_recv, piece_send, piece_recv, in_sem, out_sem,
):
    me = lax.axis_index("kv")
    my_tp = lax.axis_index("tp")
    toks = own * BLK
    pos = li_ref.shape[1]
    pairs = own // PAIR
    wide = PAIR * BLK
    far_rows = MOST * BLK
    scale = hd**-0.5
    log2e = math.log2(math.e)

    barrier = pltpu.get_barrier_semaphore()
    loop(1, devs, lambda d: pl.semaphore_signal(
        barrier, inc=1, device_id={"kv": lax.rem(me + d, devs)}, device_id_type=MESH
    ))
    for d in range(1, tps):
        pl.semaphore_signal(
            barrier, inc=1, device_id={"tp": lax.rem(my_tp + d, tps)}, device_id_type=MESH
        )

    def ask(m, src):
        return pltpu.make_async_remote_copy(
            src_ref=hot_ref.at[m], dst_ref=asked_ref.at[src],
            send_sem=hot_send.at[m], recv_sem=hot_recv.at[src],
            device_id={"kv": m}, device_id_type=MESH,
        )

    def answer(s, n, src):
        return pltpu.make_async_remote_copy(
            src_ref=reply_ref.at[s, n], dst_ref=far_ref.at[s, src],
            send_sem=far_send.at[s, n], recv_sem=far_recv.at[s, src],
            device_id={"kv": n}, device_id_type=MESH,
        )

    def columns(g, t):
        return at(g * tps + t if groups == devs else t * groups + g, share)

    def shuffle(g, t, src):
        return pltpu.make_async_remote_copy(
            src_ref=li_ref.at[:, :, columns(g, t)],
            dst_ref=rows_ref.at[g, :, at(src, pos), :],
            send_sem=li_send.at[t, g], recv_sem=li_recv.at[src, g],
            device_id={"tp": t}, device_id_type=MESH,
        )

    def keep(g):
        return pltpu.make_async_copy(
            li_ref.at[:, :, columns(g, my_tp)], rows_ref.at[g, :, at(my_tp, pos), :], li_sem.at[g]
        )

    def back(s, m, src):
        return pltpu.make_async_remote_copy(
            src_ref=out_ref.at[s, m], dst_ref=back_ref.at[s, src],
            send_sem=back_send.at[s, m], recv_sem=back_recv.at[s, src],
            device_id={"kv": m}, device_id_type=MESH,
        )

    def spread(s, t, src):
        return pltpu.make_async_remote_copy(
            src_ref=vg_ref.at[s, at(src, hd), :], dst_ref=vg_ref.at[s, at(src, hd), :],
            send_sem=vg_send.at[s, t], recv_sem=vg_recv.at[s, src],
            device_id={"tp": t}, device_id_type=MESH,
        )

    def piece(kv, src):
        return pltpu.make_async_remote_copy(
            src_ref=part_ref.at[kv], dst_ref=piece_ref.at[src],
            send_sem=piece_send.at[kv], recv_sem=piece_recv.at[src],
            device_id={"kv": kv}, device_id_type=MESH,
        )

    ins = [
        pltpu.make_async_copy(src, dst, in_sem.at[i])
        for i, (src, dst) in enumerate(
            [(k_in, k_ref), (v_in, v_ref), (g_in, g_ref), (q_in, q_ref), (c_in, c_ref)]
        )
    ]
    for copy in ins:
        copy.start()

    def put(i, src, dst):
        return pltpu.make_async_copy(src, dst, out_sem.at[i])

    peers = [lax.rem(my_tp + d, tps) for d in range(1, tps)]

    count = devs * SUB
    row = lax.broadcasted_iota(jnp.int32, (count, LANES), 0)
    lane = lax.broadcasted_iota(jnp.int32, (devs, LANES), 1)
    holder, inner = row // SUB, row % SUB
    block = jnp.where(inner < own, holder * own + inner, -1)
    topk = chosen_ref.shape[3]
    across = lax.broadcasted_iota(jnp.int32, (count, count), 1)
    down = lax.broadcasted_iota(jnp.int32, (count, count), 0)
    lower = jnp.where((across // SUB == down // SUB) & (across < down), 1.0, 0.0).astype(BF)
    for s in range(seqs):
        seen = jnp.zeros((count, LANES), F32)
        named = []
        for b in range(own):
            hit = jnp.where(block[:, :topk] == chosen_ref[s, b], 1.0, 0.0)
            hit = jnp.broadcast_to(jnp.max(hit, axis=1, keepdims=True), (count, LANES))
            named_ref[s * own + b] = hit.reshape(devs, SUB, LANES)
            named.append(hit)
            seen = jnp.maximum(seen, hit)
        seen = jnp.where(holder < me, seen, 0.0)
        rank = jnp.dot(lower, seen.astype(BF), preferred_element_type=F32)
        for j in range(MOST):
            hot = jnp.where(rank == j, seen, 0.0)
            hot_ref[:, s, j] = hot.reshape(devs, SUB, LANES)
            oks = [jnp.sum((hot * n).reshape(devs, SUB, LANES), axis=1) for n in named]
            for t in range(pairs):
                ok = jnp.where(lane < BLK, oks[PAIR * t], oks[PAIR * t + 1])
                farb_ref[s * pairs + t, j] = (1.0 - ok) * NEG
        for t in range(pairs):
            ok = jnp.where(
                lane[:SUB] < BLK,
                named_ref[s * own + PAIR * t, me],
                named_ref[s * own + PAIR * t + 1, me],
            )
            nearb_ref[s * pairs + t] = (1.0 - ok) * NEG

    pl.semaphore_wait(barrier, devs - 1 + tps - 1)
    loop(0, me, lambda m: ask(m, me).start())

    for copy in ins:
        copy.wait()
    for s in range(seqs):
        near_ref[s] = jnp.concatenate([k_ref[s], v_ref[s]], axis=0).T
        gate_ref[s] = jax.nn.sigmoid(g_ref[s]).T

    def blank(m):
        for s in range(seqs):
            far_ref[s, m] = jnp.zeros(far_ref.shape[2:], BF)

    loop(me, devs - 1, blank)

    for s in range(seqs):

        def reply(i):
            n = devs - 1 - i
            if s == 0:
                ask(0, n).wait_recv()
            for j in range(MOST):
                total = None
                for b in range(own):
                    one = asked_ref[n, s, j, b : b + 1, :].astype(BF)
                    term = one * near_ref[s, b * BLK : (b + 1) * BLK, :]
                    total = term if total is None else total + term
                reply_ref[s, n, j * BLK : (j + 1) * BLK, :] = total
            answer(s, n, me).start()

        loop(0, devs - 1 - me, reply)

    for t in peers:
        loop(0, groups, lambda g: shuffle(g, t, my_tp).start())
    loop(0, groups, lambda g: keep(g).start())

    chunks = devs - 1
    rows = heads * wide

    def attention(s):
        loop(0, me, lambda m: answer(s, 0, m).wait_recv())

        def turn(m, carry):
            kt_ref[:, at(m, far_rows)] = (far_ref[s, m][:, :hd] * scale).astype(BF).T
            return carry

        fold(chunks, turn, 0)
        for c in range(pairs):
            kt_ref[:, chunks * far_rows + c * wide : chunks * far_rows + (c + 1) * wide] = (
                (near_ref[s, c * wide : (c + 1) * wide, :hd] * scale).astype(BF).T
            )

        for t in range(pairs):
            tok = slice(t * wide, (t + 1) * wide)
            q = (q_ref[s, tok, :].astype(F32) * scale).astype(BF)
            cot = c_ref[s, tok, :].astype(F32)
            gate = gate_ref[s, tok, :]
            zero = jnp.zeros((rows, hd), BF)
            qs = jnp.concatenate([q[:, h * hd : (h + 1) * hd] for h in range(heads)], axis=0)
            bg = jnp.concatenate(
                [gate[:, h : h + 1] * cot[:, h * hd : (h + 1) * hd] for h in range(heads)], axis=0
            ).astype(BF)
            qs = jnp.concatenate([qs, zero], axis=1)
            bg = jnp.concatenate([zero, bg], axis=1)
            dims = (((1,), (1,)), ((), ()))
            ahead = lax.broadcasted_iota(jnp.int32, (wide, rows), 0) <= lax.rem(
                lax.broadcasted_iota(jnp.int32, (wide, rows), 1), wide
            )
            st = s * pairs + t

            def load(kind, c):
                return far_ref[s, c] if kind else near_ref[s, c * wide : (c + 1) * wide, :]

            def place(kind, c):
                return at(c, far_rows) if kind else slice(
                    chunks * far_rows + c * wide, chunks * far_rows + (c + 1) * wide
                )

            def score(kind, c, top):
                kv = load(kind, c)
                raw = lax.dot_general(kv, qs, dims, preferred_element_type=F32) * log2e
                w_ref[place(kind, c), :] = lax.dot_general(kv, bg, dims, preferred_element_type=F32)
                halves = []
                for j in range(MOST if kind else PAIR):
                    if kind:
                        bias = farb_ref[st, j, pl.ds(c, 1), :]
                    else:
                        bias = nearb_ref[st, c * PAIR + j : c * PAIR + j + 1, :]
                    bias = jnp.concatenate([bias] * heads, axis=1)
                    halves.append(raw[j * BLK : (j + 1) * BLK] + bias)
                sc = jnp.concatenate(halves, axis=0)
                if not kind and c == t:
                    sc = jnp.where(ahead, sc, NEG)
                s_ref[place(kind, c), :] = sc
                return jnp.maximum(top, jnp.max(sc.reshape(-1, SUB, rows), axis=0))

            top = jnp.full((SUB, rows), NEG, F32)
            for c in range(t + 1):
                top = score(False, c, top)
            top = fold(chunks, functools.partial(score, True), top)
            top = jnp.max(top, axis=0, keepdims=True)

            def weigh(kind, c, carry):
                norm, dot = carry
                p = jnp.exp2(s_ref[place(kind, c), :] - top)
                s_ref[place(kind, c), :] = p
                norm += jnp.sum(p.reshape(-1, SUB, rows), axis=0)
                dot += jnp.sum((p * w_ref[place(kind, c), :]).reshape(-1, SUB, rows), axis=0)
                return norm, dot

            carry = (jnp.zeros((SUB, rows), F32), jnp.zeros((SUB, rows), F32))
            for c in range(t + 1):
                carry = weigh(False, c, carry)
            norm, dot = fold(chunks, functools.partial(weigh, True), carry)
            inv = 1.0 / jnp.sum(norm, axis=0, keepdims=True)
            dot = jnp.sum(dot, axis=0, keepdims=True) * inv

            def grad(kind, c, carry):
                w = s_ref[place(kind, c), :] * inv
                ds = (w * (w_ref[place(kind, c), :] - dot)).astype(BF)
                ds_ref[place(kind, c), :] = ds
                more = jnp.dot(ds, qs, preferred_element_type=F32)
                more += jnp.dot(w.astype(BF), bg, preferred_element_type=F32)
                if t == 0 or (not kind and c == t):
                    dkv_ref[place(kind, c), :] = more
                else:
                    dkv_ref[place(kind, c), :] += more
                return carry

            for c in range(t + 1):
                grad(False, c, 0)
            fold(chunks, functools.partial(grad, True), 0)
            used = chunks * far_rows + (t + 1) * wide
            dqt = jnp.dot(kt_ref[:, :used], ds_ref[:used, :], preferred_element_type=F32)
            dqt = jnp.concatenate([dqt[:, h * wide : (h + 1) * wide] for h in range(heads)], axis=0)
            dq_ref[s, tok, :] = dqt.T.astype(BF)

        def give(m):
            out_ref[s, m] = dkv_ref[at(m, far_rows), :].astype(BF)
            back(s, m, me).start()

        loop(0, me, give)
        total_ref[s] = dkv_ref[chunks * far_rows :, :]

    loop(0, seqs, attention)
    puts = [put(0, dq_ref, dq_out)]
    puts[0].start()

    def product(s, g):
        return jnp.dot(vg_ref[s], rows_ref[g, s], preferred_element_type=F32)

    for t in peers:
        loop(0, groups, lambda g: shuffle(g, t, t).wait_recv())
    loop(0, groups, lambda g: keep(g).wait())
    for s in range(seqs):

        def add(n):
            back(s, 0, n).wait_recv()
            for b in range(own):
                term = None
                for j in range(MOST):
                    one = asked_ref[n, s, j, b : b + 1, :]
                    more = one * back_ref[s, n, j * BLK : (j + 1) * BLK, :].astype(F32)
                    term = more if term is None else term + more
                total_ref[s, b * BLK : (b + 1) * BLK, :] += term

        loop(me + 1, devs, add)
        both = total_ref[s].T.astype(BF)
        kg_ref[s] = both[:hd]
        vo_ref[s] = both[hd:]
        vg_ref[s, at(my_tp, hd), :] = both[hd:]
        for t in peers:
            spread(s, t, my_tp).start()
        if s < seqs - 1:
            for t in peers:
                spread(s, t, t).wait_recv()

            def early(g):
                if s == 0:
                    acc_ref[g] = product(s, g)
                else:
                    acc_ref[g] += product(s, g)

            loop(0, groups, early)

    for out in [put(1, kg_ref, kg_out), put(2, vo_ref, vo_out)]:
        out.start()
        puts.append(out)
    for t in peers:
        spread(seqs - 1, t, t).wait_recv()

    def other(i):
        low = devs - 1 - i
        low = jnp.where(low > me, low, low - 1)
        high = jnp.where(i < me, i, i + 1)
        return jnp.where(me * 2 < devs, low, high)

    def final(g):
        last = product(seqs - 1, g)
        return last if seqs == 1 else last + acc_ref[g]

    if groups == devs:

        def stage(i):
            kv = other(i)
            part_ref[kv] = final(kv).astype(BF)
            piece(kv, me).start()

        loop(0, devs - 1, stage)
        part_ref[me] = final(me).astype(BF)
    else:
        each = devs // groups

        def stage(g):
            part_ref[pl.ds(g * each, each)] = final(g).T.astype(BF).reshape((each,) + part_ref.shape[1:])

        loop(0, groups, stage)
        loop(0, devs - 1, lambda i: piece(other(i), me).start())
    piece_ref[me] = part_ref[me]

    def arrive(i):
        piece(0, other(i)).wait_recv()

    loop(0, devs - 1, arrive)
    result = piece_ref[0].astype(F32)
    for n in range(1, devs):
        result += piece_ref[n].astype(F32)
    wg_ref[...] = result.T if groups == devs else result
    puts.append(put(3, wg_ref, wg_out))
    puts[-1].start()

    loop(0, me, lambda m: ask(m, me).wait_send())
    for t in peers:
        loop(0, groups, lambda g: shuffle(g, t, my_tp).wait_send())
    for s in range(seqs):
        loop(me + 1, devs, lambda n: answer(s, n, me).wait_send())
        loop(0, me, lambda m: back(s, m, me).wait_send())
        for t in peers:
            spread(s, t, my_tp).wait_send()
    loop(0, devs - 1, lambda i: piece(other(i), me).wait_send())
    for out in puts:
        out.wait()


def leave(count, *refs):
    ins, outs, held = refs[:count], refs[count : 2 * count], refs[2 * count : 3 * count]
    sems = refs[3 * count]
    reads = [pltpu.make_async_copy(ins[i], held[i], sems.at[0, i]) for i in range(count)]
    writes = [pltpu.make_async_copy(held[i], outs[i], sems.at[1, i]) for i in range(count)]
    for read in reads:
        read.start()
    for read, write in zip(reads, writes):
        read.wait()
        write.start()
    for write in writes:
        write.wait()


def on_device(queries, key_states, value_states, cotangent, gate_logits, layer_input, chosen):
    seqs, toks, width = queries.shape
    hd = key_states.shape[2]
    heads = width // hd
    own = toks // BLK
    pairs = own // PAIR
    devs = lax.axis_size("kv")
    tps = lax.axis_size("tp")
    pos = layer_input.shape[1]
    share = layer_input.shape[2] // (devs * tps)
    groups, cut = devs, share
    if share % LANES:
        groups, cut = devs * share // LANES, LANES
        layer_input = layer_input.reshape(seqs, pos, devs, tps, share)
        layer_input = jnp.swapaxes(layer_input, 2, 3).reshape(seqs, pos, devs * tps * share)
    part = (tps * hd, share) if groups == devs else (share, tps * hd)
    keys = (devs - 1) * MOST * BLK + toks
    rows = heads * PAIR * BLK
    sent = (MOST * BLK, 2 * hd)

    vmem = pl.BlockSpec(memory_space=pltpu.VMEM)
    hbm = pl.BlockSpec(memory_space=pl.ANY)
    dma = pltpu.SemaphoreType.DMA
    results = pl.pallas_call(
        functools.partial(whole, devs, tps, seqs, own, heads, hd, cut, groups),
        in_specs=[vmem] + [hbm] * 6,
        out_specs=[hbm] * 4,
        out_shape=[
            jax.ShapeDtypeStruct((seqs, toks, width), BF),
            jax.ShapeDtypeStruct((seqs, hd, toks), BF),
            jax.ShapeDtypeStruct((seqs, hd, toks), BF),
            jax.ShapeDtypeStruct((share, tps * hd), F32),
        ],
        scratch_shapes=[
            pltpu.VMEM((seqs, toks, width), BF),
            pltpu.VMEM((seqs, toks, width), BF),
            pltpu.VMEM((seqs, heads, toks), F32),
            pltpu.VMEM((seqs, hd, toks), BF),
            pltpu.VMEM((seqs, hd, toks), BF),
            pltpu.VMEM((seqs, toks, width), BF),
            pltpu.VMEM((seqs, hd, toks), BF),
            pltpu.VMEM((seqs, hd, toks), BF),
            pltpu.VMEM((share, tps * hd), F32),
            pltpu.VMEM((seqs, toks, 2 * hd), BF),
            pltpu.VMEM((seqs, toks, heads), F32),
            pltpu.VMEM((seqs * own, devs, SUB, LANES), F32),
            pltpu.VMEM((devs, seqs, MOST, SUB, LANES), F32),
            pltpu.VMEM((devs, seqs, MOST, SUB, LANES), F32),
            pltpu.VMEM((seqs * pairs, MOST, devs, LANES), F32),
            pltpu.VMEM((seqs * pairs, SUB, LANES), F32),
            pltpu.VMEM((seqs, devs) + sent, BF),
            pltpu.VMEM((seqs, devs - 1) + sent, BF),
            pltpu.VMEM((groups, seqs, toks, cut), BF),
            pltpu.VMEM((hd, keys), BF),
            pltpu.VMEM((keys, rows), F32),
            pltpu.VMEM((keys, rows), F32),
            pltpu.VMEM((keys, rows), BF),
            pltpu.VMEM((keys, 2 * hd), F32),
            pltpu.VMEM((seqs, devs - 1) + sent, BF),
            pltpu.VMEM((seqs, toks, 2 * hd), F32),
            pltpu.VMEM((seqs, devs) + sent, BF),
            pltpu.VMEM((seqs, tps * hd, toks), BF),
            pltpu.VMEM((groups, tps * hd, cut), F32),
            pltpu.VMEM((devs,) + part, BF),
            pltpu.VMEM((devs,) + part, BF),
            dma((devs,)), dma((devs,)),
            dma((seqs, devs)), dma((seqs, devs)),
            dma((tps, groups)), dma((tps, groups)), dma((groups,)),
            dma((seqs, devs)), dma((seqs, devs)),
            dma((seqs, tps)), dma((seqs, tps)),
            dma((devs,)), dma((devs,)),
            dma((5,)), dma((4,)),
        ],
        compiler_params=pltpu.CompilerParams(
            collective_id=0, has_side_effects=True, vmem_limit_bytes=60 * 2**20
        ),
    )(
        chosen, queries, cotangent, jnp.swapaxes(gate_logits, 1, 2),
        jnp.swapaxes(key_states, 1, 2), jnp.swapaxes(value_states, 1, 2), layer_input,
    )
    query_grad, key_grad, value_grad, weight_grad = pl.pallas_call(
        functools.partial(leave, len(results)),
        in_specs=[hbm] * len(results),
        out_specs=[hbm] * len(results),
        out_shape=[jax.ShapeDtypeStruct(r.shape, r.dtype) for r in results],
        scratch_shapes=[pltpu.VMEM(r.shape, r.dtype) for r in results] + [dma((2, len(results)))],
        compiler_params=pltpu.CompilerParams(vmem_limit_bytes=60 * 2**20),
    )(*results)
    return query_grad, jnp.swapaxes(key_grad, 1, 2), jnp.swapaxes(value_grad, 1, 2), weight_grad


def solution(mesh):
    in_specs = (
        P(None, "kv", "tp"),
        P(None, "kv", "tp"),
        P(None, "kv", "tp"),
        P(None, "kv", "tp"),
        P(None, "kv", "tp"),
        P(None, ("kv", "tp"), None),
        P(None, "kv", "tp", None),
    )
    out_specs = (
        P(None, "kv", "tp"),
        P(None, "kv", "tp"),
        P(None, "kv", "tp"),
        P(("kv", "tp"), None),
    )
    return jax.shard_map(
        on_device, mesh=mesh, in_specs=in_specs, out_specs=out_specs, check_vma=False
    )
```

```python
import functools
import math

import jax
import jax.numpy as jnp
from jax import lax
from jax.experimental import pallas as pl
from jax.experimental.pallas import tpu as pltpu
from jax.sharding import PartitionSpec as P

BLK = 64
MOST = 2
PAIR = 2
SUB = 8
LANES = 128
NEG = -1e30
MESH = pl.DeviceIdType.MESH
BF = jnp.bfloat16
F32 = jnp.float32


def loop(lo, hi, body):
    def step(i, carry):
        body(i)
        return carry

    lax.fori_loop(lo, hi, step, 0)


def at(i, size):
    return pl.ds(i * size, size) if isinstance(i, int) else pl.ds(pl.multiple_of(i * size, size), size)


def whole(
    devs, tps, seqs, own, heads, hd, share, groups,
    chosen_ref, q_in, c_in, g_in, k_in, v_in, li_ref,
    dq_out, kg_out, vo_out, wg_out,
    q_ref, c_ref, g_ref, k_ref, v_ref, dq_ref, kg_ref, vo_ref, wg_ref,
    near_ref, gate_ref, named_ref, hot_ref, asked_ref, farb_ref, nearb_ref,
    reply_ref, far_ref, rows_ref, qs_ref, bg_ref, s_ref, w_ref, top_ref, dqt_ref,
    out_ref, total_ref, back_ref, vg_ref, acc_ref, part_ref, piece_ref,
    hot_send, hot_recv, far_send, far_recv, li_send, li_recv, li_sem,
    back_send, back_recv, vg_send, vg_recv, piece_send, piece_recv, in_sem, out_sem,
):
    me = lax.axis_index("kv")
    my_tp = lax.axis_index("tp")
    toks = own * BLK
    pos = li_ref.shape[1]
    pairs = own // PAIR
    wide = PAIR * BLK
    far_rows = MOST * BLK
    scale = hd**-0.5
    log2e = math.log2(math.e)

    barrier = pltpu.get_barrier_semaphore()
    loop(1, devs, lambda d: pl.semaphore_signal(
        barrier, inc=1, device_id={"kv": lax.rem(me + d, devs)}, device_id_type=MESH
    ))
    for d in range(1, tps):
        pl.semaphore_signal(
            barrier, inc=1, device_id={"tp": lax.rem(my_tp + d, tps)}, device_id_type=MESH
        )

    def ask(m, src):
        return pltpu.make_async_remote_copy(
            src_ref=hot_ref.at[m], dst_ref=asked_ref.at[src],
            send_sem=hot_send.at[m], recv_sem=hot_recv.at[src],
            device_id={"kv": m}, device_id_type=MESH,
        )

    def answer(s, n, src):
        return pltpu.make_async_remote_copy(
            src_ref=reply_ref.at[s, n], dst_ref=far_ref.at[s, src],
            send_sem=far_send.at[s, n], recv_sem=far_recv.at[s, src],
            device_id={"kv": n}, device_id_type=MESH,
        )

    def columns(g, t):
        return at(g * tps + t if groups == devs else t * groups + g, share)

    def shuffle(g, t, src):
        return pltpu.make_async_remote_copy(
            src_ref=li_ref.at[:, :, columns(g, t)],
            dst_ref=rows_ref.at[g, :, at(src, pos), :],
            send_sem=li_send.at[t, g], recv_sem=li_recv.at[src, g],
            device_id={"tp": t}, device_id_type=MESH,
        )

    def keep(g):
        return pltpu.make_async_copy(
            li_ref.at[:, :, columns(g, my_tp)], rows_ref.at[g, :, at(my_tp, pos), :], li_sem.at[g]
        )

    def back(s, m, src):
        return pltpu.make_async_remote_copy(
            src_ref=out_ref.at[s, m], dst_ref=back_ref.at[s, src],
            send_sem=back_send.at[s, m], recv_sem=back_recv.at[s, src],
            device_id={"kv": m}, device_id_type=MESH,
        )

    def spread(s, t, src):
        return pltpu.make_async_remote_copy(
            src_ref=vg_ref.at[s, at(src, hd), :], dst_ref=vg_ref.at[s, at(src, hd), :],
            send_sem=vg_send.at[s, t], recv_sem=vg_recv.at[s, src],
            device_id={"tp": t}, device_id_type=MESH,
        )

    def piece(kv, src):
        return pltpu.make_async_remote_copy(
            src_ref=part_ref.at[kv], dst_ref=piece_ref.at[src],
            send_sem=piece_send.at[kv], recv_sem=piece_recv.at[src],
            device_id={"kv": kv}, device_id_type=MESH,
        )

    ins = [
        pltpu.make_async_copy(src, dst, in_sem.at[i])
        for i, (src, dst) in enumerate(
            [(k_in, k_ref), (v_in, v_ref), (g_in, g_ref), (q_in, q_ref), (c_in, c_ref)]
        )
    ]
    for copy in ins:
        copy.start()

    def put(i, src, dst):
        return pltpu.make_async_copy(src, dst, out_sem.at[i])

    peers = [lax.rem(my_tp + d, tps) for d in range(1, tps)]

    count = devs * SUB
    row = lax.broadcasted_iota(jnp.int32, (count, LANES), 0)
    lane = lax.broadcasted_iota(jnp.int32, (devs, LANES), 1)
    holder, inner = row // SUB, row % SUB
    block = jnp.where(inner < own, holder * own + inner, -1)
    topk = chosen_ref.shape[3]
    across = lax.broadcasted_iota(jnp.int32, (count, count), 1)
    down = lax.broadcasted_iota(jnp.int32, (count, count), 0)
    lower = jnp.where((across // SUB == down // SUB) & (across < down), 1.0, 0.0).astype(BF)
    for s in range(seqs):
        seen = jnp.zeros((count, LANES), F32)
        named = []
        for b in range(own):
            hit = jnp.where(block[:, :topk] == chosen_ref[s, b], 1.0, 0.0)
            hit = jnp.broadcast_to(jnp.max(hit, axis=1, keepdims=True), (count, LANES))
            named_ref[s * own + b] = hit.reshape(devs, SUB, LANES)
            named.append(hit)
            seen = jnp.maximum(seen, hit)
        seen = jnp.where(holder < me, seen, 0.0)
        rank = jnp.dot(lower, seen.astype(BF), preferred_element_type=F32)
        for j in range(MOST):
            hot = jnp.where(rank == j, seen, 0.0)
            hot_ref[:, s, j] = hot.reshape(devs, SUB, LANES)
            oks = [jnp.sum((hot * n).reshape(devs, SUB, LANES), axis=1) for n in named]
            for t in range(pairs):
                ok = jnp.where(lane < BLK, oks[PAIR * t], oks[PAIR * t + 1])
                farb_ref[s * pairs + t, j] = (1.0 - ok) * NEG
        for t in range(pairs):
            ok = jnp.where(
                lane[:SUB] < BLK,
                named_ref[s * own + PAIR * t, me],
                named_ref[s * own + PAIR * t + 1, me],
            )
            nearb_ref[s * pairs + t] = (1.0 - ok) * NEG

    pl.semaphore_wait(barrier, devs - 1 + tps - 1)
    loop(0, me, lambda m: ask(m, me).start())

    for copy in ins:
        copy.wait()
    for s in range(seqs):
        near_ref[s] = jnp.concatenate([k_ref[s], v_ref[s]], axis=0).T
        gate_ref[s] = jax.nn.sigmoid(g_ref[s]).T

    def reply(s, i):
        n = devs - 1 - i
        for j in range(MOST):
            total = None
            for b in range(own):
                one = asked_ref[n, s, j, b : b + 1, :].astype(BF)
                term = one * near_ref[s, b * BLK : (b + 1) * BLK, :]
                total = term if total is None else total + term
            reply_ref[s, n, j * BLK : (j + 1) * BLK, :] = total
        answer(s, n, me).start()

    def first(i):
        ask(0, devs - 1 - i).wait_recv()
        reply(0, i)

    later = devs - 1 - me
    nearest = jnp.minimum(max(devs // 4, 1), later)
    loop(0, nearest, first)

    for t in peers:
        loop(0, groups, lambda g: shuffle(g, t, my_tp).start())
    loop(0, groups, lambda g: keep(g).start())

    chunks = devs - 1
    rows = heads * wide
    dims = (((1,), (1,)), ((), ()))
    ahead = lax.broadcasted_iota(jnp.int32, (wide, rows), 0) <= lax.rem(
        lax.broadcasted_iota(jnp.int32, (wide, rows), 1), wide
    )

    def settle(s):
        def add(n):
            back(s, 0, n).wait_recv()
            for b in range(own):
                term = None
                for j in range(MOST):
                    one = asked_ref[n, s, j, b : b + 1, :]
                    more = one * back_ref[s, n, j * BLK : (j + 1) * BLK, :].astype(F32)
                    term = more if term is None else term + more
                total_ref[s, b * BLK : (b + 1) * BLK, :] += term

        loop(me + 1, devs, add)
        both = total_ref[s].T.astype(BF)
        kg_ref[s] = both[:hd]
        vo_ref[s] = both[hd:]
        vg_ref[s, at(my_tp, hd), :] = both[hd:]
        for t in peers:
            spread(s, t, my_tp).start()

    def attention(s):
        for t in range(pairs):
            tok = slice(t * wide, (t + 1) * wide)
            q = (q_ref[s, tok, :].astype(F32) * scale).astype(BF)
            cot = c_ref[s, tok, :].astype(F32)
            gate = gate_ref[s, tok, :]
            zero = jnp.zeros((rows, hd), BF)
            qs = jnp.concatenate([q[:, h * hd : (h + 1) * hd] for h in range(heads)], axis=0)
            bg = jnp.concatenate(
                [gate[:, h : h + 1] * cot[:, h * hd : (h + 1) * hd] for h in range(heads)], axis=0
            ).astype(BF)
            qs_ref[t] = jnp.concatenate([qs, zero], axis=1)
            bg_ref[t] = jnp.concatenate([zero, bg], axis=1)

        def score(kv, t, chunk, bias, diagonal, carry):
            top, norm, dot = carry
            raw = lax.dot_general(kv, qs_ref[t], dims, preferred_element_type=F32) * log2e
            wg = lax.dot_general(kv, bg_ref[t], dims, preferred_element_type=F32)
            sc = jnp.concatenate(
                [
                    raw[j * BLK : (j + 1) * BLK] + jnp.concatenate([b] * heads, axis=1)
                    for j, b in enumerate(bias)
                ],
                axis=0,
            )
            if diagonal:
                sc = jnp.where(ahead, sc, NEG)
            peak = jnp.maximum(top, jnp.max(sc, axis=0, keepdims=True))
            p = jnp.exp2(sc - peak)
            less = jnp.exp2(top - peak)
            s_ref[chunk, :, t * rows : (t + 1) * rows] = p.astype(s_ref.dtype)
            w_ref[chunk, :, t * rows : (t + 1) * rows] = wg
            top_ref[chunk, :, t * rows : (t + 1) * rows] = peak
            norm = norm * less + jnp.sum(p, axis=0, keepdims=True)
            dot = dot * less + jnp.sum(p * wg, axis=0, keepdims=True)
            return peak, norm, dot

        carries = []
        for t in range(pairs):
            carry = (jnp.full((1, rows), NEG, F32), jnp.zeros((1, rows), F32), jnp.zeros((1, rows), F32))
            for c in range(t, -1, -1):
                kv = near_ref[s, c * wide : (c + 1) * wide, :]
                bias = [
                    nearb_ref[s * pairs + t, c * PAIR + j : c * PAIR + j + 1, :] for j in range(PAIR)
                ]
                carry = score(kv, t, chunks + c, bias, c == t, carry)
            carries.append(carry)

        @pl.when(s == 0)
        def _():
            loop(nearest, later, first)

        def forth(i, carries):
            m = me - 1 - i
            answer(s, 0, m).wait_recv()
            kv = far_ref[s, m]
            return tuple(
                score(
                    kv, t, m,
                    [farb_ref[s * pairs + t, j, pl.ds(m, 1), :] for j in range(MOST)],
                    False, carries[t],
                )
                for t in range(pairs)
            )

        carries = lax.fori_loop(0, me, forth, tuple(carries))

        @pl.when((s < seqs - 1) & (me * 2 >= devs))
        def _():
            loop(0, later, functools.partial(reply, s + 1))

        @pl.when(s > 0)
        def _():
            settle(s - 1)

        tops = [carry[0] for carry in carries]
        invs = [1.0 / carry[1] for carry in carries]
        dots = [carry[2] * inv for carry, inv in zip(carries, invs)]
        dqt_ref[...] = jnp.zeros_like(dqt_ref)

        def grad(kv, chunk, ts):
            kt = (kv[:, :hd] * scale).astype(BF).T
            total = None
            for t in ts:
                cols = slice(t * rows, (t + 1) * rows)
                part = jnp.exp2(top_ref[chunk, :, cols] - tops[t]) * invs[t]
                w = s_ref[chunk, :, cols].astype(F32) * part
                ds = (w * (w_ref[chunk, :, cols] - dots[t])).astype(BF)
                more = jnp.dot(ds, qs_ref[t], preferred_element_type=F32)
                more += jnp.dot(w.astype(BF), bg_ref[t], preferred_element_type=F32)
                total = more if total is None else total + more
                dqt_ref[:, cols] += jnp.dot(kt, ds, preferred_element_type=F32)
            return total

        def give(m):
            out_ref[s, m] = grad(far_ref[s, m], m, range(pairs)).astype(BF)
            back(s, m, me).start()

        loop(0, me, give)
        for c in range(pairs):
            kv = near_ref[s, c * wide : (c + 1) * wide, :]
            total_ref[s, c * wide : (c + 1) * wide, :] = grad(kv, chunks + c, range(c, pairs))
        for t in range(pairs):
            dqt = dqt_ref[:, t * rows : (t + 1) * rows]
            dqt = jnp.concatenate([dqt[:, h * wide : (h + 1) * wide] for h in range(heads)], axis=0)
            dq_ref[s, t * wide : (t + 1) * wide, :] = dqt.T.astype(BF)

        @pl.when((s < seqs - 1) & (me * 2 < devs))
        def _():
            loop(0, later, functools.partial(reply, s + 1))

    loop(0, seqs, attention)
    puts = [put(0, dq_ref, dq_out)]
    puts[0].start()

    def product(s, g):
        return jnp.dot(vg_ref[s], rows_ref[g, s], preferred_element_type=F32)

    settle(seqs - 1)
    for t in peers:
        loop(0, groups, lambda g: shuffle(g, t, t).wait_recv())
    loop(0, groups, lambda g: keep(g).wait())
    for s in range(seqs - 1):
        for t in peers:
            spread(s, t, t).wait_recv()

        def early(g):
            if s == 0:
                acc_ref[g] = product(s, g)
            else:
                acc_ref[g] += product(s, g)

        loop(0, groups, early)

    for out in [put(1, kg_ref, kg_out), put(2, vo_ref, vo_out)]:
        out.start()
        puts.append(out)
    for t in peers:
        spread(seqs - 1, t, t).wait_recv()

    def other(i):
        low = devs - 1 - i
        low = jnp.where(low > me, low, low - 1)
        high = jnp.where(i < me, i, i + 1)
        return jnp.where(me * 2 < devs, low, high)

    def final(g):
        last = product(seqs - 1, g)
        return last if seqs == 1 else last + acc_ref[g]

    if groups == devs:

        def stage(i):
            kv = other(i)
            part_ref[kv] = final(kv).astype(BF)
            piece(kv, me).start()

        loop(0, devs - 1, stage)
        part_ref[me] = final(me).astype(BF)
    else:
        each = devs // groups

        def stage(g):
            part_ref[pl.ds(g * each, each)] = final(g).T.astype(BF).reshape((each,) + part_ref.shape[1:])

        loop(0, groups, stage)
        loop(0, devs - 1, lambda i: piece(other(i), me).start())
    piece_ref[me] = part_ref[me]

    def arrive(i):
        piece(0, other(i)).wait_recv()

    loop(0, devs - 1, arrive)
    result = piece_ref[0].astype(F32)
    for n in range(1, devs):
        result += piece_ref[n].astype(F32)
    wg_ref[...] = result.T if groups == devs else result
    puts.append(put(3, wg_ref, wg_out))
    puts[-1].start()

    loop(0, me, lambda m: ask(m, me).wait_send())
    for t in peers:
        loop(0, groups, lambda g: shuffle(g, t, my_tp).wait_send())
    for s in range(seqs):
        loop(me + 1, devs, lambda n: answer(s, n, me).wait_send())
        loop(0, me, lambda m: back(s, m, me).wait_send())
        for t in peers:
            spread(s, t, my_tp).wait_send()
    loop(0, devs - 1, lambda i: piece(other(i), me).wait_send())
    for out in puts:
        out.wait()


def leave(count, *refs):
    ins, outs, held = refs[:count], refs[count : 2 * count], refs[2 * count : 3 * count]
    sems = refs[3 * count]
    reads = [pltpu.make_async_copy(ins[i], held[i], sems.at[0, i]) for i in range(count)]
    writes = [pltpu.make_async_copy(held[i], outs[i], sems.at[1, i]) for i in range(count)]
    for read in reads:
        read.start()
    for read, write in zip(reads, writes):
        read.wait()
        write.start()
    for write in writes:
        write.wait()


def on_device(queries, key_states, value_states, cotangent, gate_logits, layer_input, chosen):
    seqs, toks, width = queries.shape
    hd = key_states.shape[2]
    heads = width // hd
    own = toks // BLK
    pairs = own // PAIR
    devs = lax.axis_size("kv")
    tps = lax.axis_size("tp")
    pos = layer_input.shape[1]
    share = layer_input.shape[2] // (devs * tps)
    groups, cut = devs, share
    if share % LANES:
        groups, cut = devs * share // LANES, LANES
        layer_input = layer_input.reshape(seqs, pos, devs, tps, share)
        layer_input = jnp.swapaxes(layer_input, 2, 3).reshape(seqs, pos, devs * tps * share)
    part = (tps * hd, share) if groups == devs else (share, tps * hd)
    chunks = devs - 1 + pairs
    rows = heads * PAIR * BLK
    scores = (chunks, PAIR * BLK, pairs * rows)
    sent = (MOST * BLK, 2 * hd)

    vmem = pl.BlockSpec(memory_space=pltpu.VMEM)
    hbm = pl.BlockSpec(memory_space=pl.ANY)
    dma = pltpu.SemaphoreType.DMA
    results = pl.pallas_call(
        functools.partial(whole, devs, tps, seqs, own, heads, hd, cut, groups),
        in_specs=[vmem] + [hbm] * 6,
        out_specs=[hbm] * 4,
        out_shape=[
            jax.ShapeDtypeStruct((seqs, toks, width), BF),
            jax.ShapeDtypeStruct((seqs, hd, toks), BF),
            jax.ShapeDtypeStruct((seqs, hd, toks), BF),
            jax.ShapeDtypeStruct((share, tps * hd), F32),
        ],
        scratch_shapes=[
            pltpu.VMEM((seqs, toks, width), BF),
            pltpu.VMEM((seqs, toks, width), BF),
            pltpu.VMEM((seqs, heads, toks), F32),
            pltpu.VMEM((seqs, hd, toks), BF),
            pltpu.VMEM((seqs, hd, toks), BF),
            pltpu.VMEM((seqs, toks, width), BF),
            pltpu.VMEM((seqs, hd, toks), BF),
            pltpu.VMEM((seqs, hd, toks), BF),
            pltpu.VMEM((share, tps * hd), F32),
            pltpu.VMEM((seqs, toks, 2 * hd), BF),
            pltpu.VMEM((seqs, toks, heads), F32),
            pltpu.VMEM((seqs * own, devs, SUB, LANES), F32),
            pltpu.VMEM((devs, seqs, MOST, SUB, LANES), F32),
            pltpu.VMEM((devs, seqs, MOST, SUB, LANES), F32),
            pltpu.VMEM((seqs * pairs, MOST, devs, LANES), F32),
            pltpu.VMEM((seqs * pairs, SUB, LANES), F32),
            pltpu.VMEM((seqs, devs) + sent, BF),
            pltpu.VMEM((seqs, devs - 1) + sent, BF),
            pltpu.VMEM((groups, seqs, toks, cut), BF),
            pltpu.VMEM((pairs, rows, 2 * hd), BF),
            pltpu.VMEM((pairs, rows, 2 * hd), BF),
            pltpu.VMEM(scores, F32 if math.prod(scores) <= 5 * 2**20 else BF),
            pltpu.VMEM(scores, F32),
            pltpu.VMEM((chunks, 1, pairs * rows), F32),
            pltpu.VMEM((hd, pairs * rows), F32),
            pltpu.VMEM((seqs, devs - 1) + sent, BF),
            pltpu.VMEM((seqs, toks, 2 * hd), F32),
            pltpu.VMEM((seqs, devs) + sent, BF),
            pltpu.VMEM((seqs, tps * hd, toks), BF),
            pltpu.VMEM((groups, tps * hd, cut), F32),
            pltpu.VMEM((devs,) + part, BF),
            pltpu.VMEM((devs,) + part, BF),
            dma((devs,)), dma((devs,)),
            dma((seqs, devs)), dma((seqs, devs)),
            dma((tps, groups)), dma((tps, groups)), dma((groups,)),
            dma((seqs, devs)), dma((seqs, devs)),
            dma((seqs, tps)), dma((seqs, tps)),
            dma((devs,)), dma((devs,)),
            dma((5,)), dma((4,)),
        ],
        compiler_params=pltpu.CompilerParams(
            collective_id=0, has_side_effects=True, vmem_limit_bytes=60 * 2**20
        ),
    )(
        chosen, queries, cotangent, jnp.swapaxes(gate_logits, 1, 2),
        jnp.swapaxes(key_states, 1, 2), jnp.swapaxes(value_states, 1, 2), layer_input,
    )
    query_grad, key_grad, value_grad, weight_grad = pl.pallas_call(
        functools.partial(leave, len(results)),
        in_specs=[hbm] * len(results),
        out_specs=[hbm] * len(results),
        out_shape=[jax.ShapeDtypeStruct(r.shape, r.dtype) for r in results],
        scratch_shapes=[pltpu.VMEM(r.shape, r.dtype) for r in results] + [dma((2, len(results)))],
        compiler_params=pltpu.CompilerParams(vmem_limit_bytes=60 * 2**20),
    )(*results)
    return query_grad, jnp.swapaxes(key_grad, 1, 2), jnp.swapaxes(value_grad, 1, 2), weight_grad


def solution(mesh):
    in_specs = (
        P(None, "kv", "tp"),
        P(None, "kv", "tp"),
        P(None, "kv", "tp"),
        P(None, "kv", "tp"),
        P(None, "kv", "tp"),
        P(None, ("kv", "tp"), None),
        P(None, "kv", "tp", None),
    )
    out_specs = (
        P(None, "kv", "tp"),
        P(None, "kv", "tp"),
        P(None, "kv", "tp"),
        P(("kv", "tp"), None),
    )
    return jax.shard_map(
        on_device, mesh=mesh, in_specs=in_specs, out_specs=out_specs, check_vma=False
    )
```

```python
import functools
import math

import jax
import jax.numpy as jnp
from jax import lax
from jax.experimental import pallas as pl
from jax.experimental.pallas import tpu as pltpu
from jax.sharding import PartitionSpec as P

BLK = 64
MOST = 2
PAIR = 2
DUO = 2
SUB = 8
LANES = 128
SPAN = 2
NEG = -1e30
MESH = pl.DeviceIdType.MESH
BF = jnp.bfloat16
F32 = jnp.float32


def loop(lo, hi, body):
    def step(i, carry):
        body(i)
        return carry

    lax.fori_loop(lo, hi, step, 0)


def at(i, size):
    return pl.ds(i * size, size) if isinstance(i, int) else pl.ds(pl.multiple_of(i * size, size), size)


def whole(
    devs, tps, seqs, own, heads, hd, share, groups,
    chosen_ref, q_in, c_in, g_in, k_in, v_in, li_ref,
    dq_out, kg_out, vo_out, wg_out,
    q_ref, c_ref, g_ref, k_ref, v_ref, dq_ref, kg_ref, vo_ref, wg_ref,
    near_ref, gate_ref, named_ref, hot_ref, asked_ref, farb_ref, nearb_ref,
    reply_ref, far_ref, rows_ref, qs_ref, bg_ref, s_ref, w_ref, top_ref, run_ref, dqt_ref,
    out_ref, total_ref, back_ref, vg_ref, acc_ref, part_ref, mate_ref, both_ref, piece_ref,
    hot_send, hot_recv, far_send, far_recv, li_send, li_recv, li_sem,
    back_send, back_recv, vg_send, vg_recv, toss_send, toss_recv, piece_send, piece_recv, in_sem, out_sem,
):
    me = lax.axis_index("kv")
    my_tp = lax.axis_index("tp")
    toks = own * BLK
    pos = li_ref.shape[1]
    pairs = own // PAIR
    wide = PAIR * BLK
    far_rows = MOST * BLK
    scale = hd**-0.5
    log2e = math.log2(math.e)

    barrier = pltpu.get_barrier_semaphore()
    loop(1, devs, lambda d: pl.semaphore_signal(
        barrier, inc=1, device_id={"kv": lax.rem(me + d, devs)}, device_id_type=MESH
    ))
    for d in range(1, tps):
        pl.semaphore_signal(
            barrier, inc=1, device_id={"tp": lax.rem(my_tp + d, tps)}, device_id_type=MESH
        )

    def ask(m, src):
        return pltpu.make_async_remote_copy(
            src_ref=hot_ref.at[m], dst_ref=asked_ref.at[src],
            send_sem=hot_send.at[m], recv_sem=hot_recv.at[src],
            device_id={"kv": m}, device_id_type=MESH,
        )

    def answer(s, n, src):
        return pltpu.make_async_remote_copy(
            src_ref=reply_ref.at[s, n], dst_ref=far_ref.at[s, src],
            send_sem=far_send.at[s, n], recv_sem=far_recv.at[s, src],
            device_id={"kv": n}, device_id_type=MESH,
        )

    def columns(g, t):
        return at(g * tps + t if groups == devs else t * groups + g, share)

    def shuffle(g, t, src):
        return pltpu.make_async_remote_copy(
            src_ref=li_ref.at[:, :, columns(g, t)],
            dst_ref=rows_ref.at[g, :, at(src, pos), :],
            send_sem=li_send.at[t, g], recv_sem=li_recv.at[src, g],
            device_id={"tp": t}, device_id_type=MESH,
        )

    def keep(g):
        return pltpu.make_async_copy(
            li_ref.at[:, :, columns(g, my_tp)], rows_ref.at[g, :, at(my_tp, pos), :], li_sem.at[g]
        )

    def back(s, m, src):
        return pltpu.make_async_remote_copy(
            src_ref=out_ref.at[s, m], dst_ref=back_ref.at[s, src],
            send_sem=back_send.at[s, m], recv_sem=back_recv.at[s, src],
            device_id={"kv": m}, device_id_type=MESH,
        )

    def spread(s, t, src):
        return pltpu.make_async_remote_copy(
            src_ref=vg_ref.at[s, at(src, hd), :], dst_ref=vg_ref.at[s, at(src, hd), :],
            send_sem=vg_send.at[s, t], recv_sem=vg_recv.at[s, src],
            device_id={"tp": t}, device_id_type=MESH,
        )

    halves, mine, my_u = devs // DUO, me // DUO, me % DUO

    def toss(g):
        return pltpu.make_async_remote_copy(
            src_ref=part_ref.at[g * DUO + 1 - my_u], dst_ref=mate_ref.at[g],
            send_sem=toss_send.at[g], recv_sem=toss_recv.at[g],
            device_id={"kv": me + 1 - 2 * my_u}, device_id_type=MESH,
        )

    def piece(g, src):
        return pltpu.make_async_remote_copy(
            src_ref=both_ref.at[g], dst_ref=piece_ref.at[src],
            send_sem=piece_send.at[g], recv_sem=piece_recv.at[src],
            device_id={"kv": g * DUO + my_u}, device_id_type=MESH,
        )

    ins = [
        pltpu.make_async_copy(src, dst, in_sem.at[i])
        for i, (src, dst) in enumerate(
            [(k_in, k_ref), (v_in, v_ref), (g_in, g_ref), (q_in, q_ref), (c_in, c_ref)]
        )
    ]
    for copy in ins:
        copy.start()

    def put(i, src, dst):
        return pltpu.make_async_copy(src, dst, out_sem.at[i])

    peers = [lax.rem(my_tp + d, tps) for d in range(1, tps)]

    count = devs * SUB
    row = lax.broadcasted_iota(jnp.int32, (count, LANES), 0)
    lane = lax.broadcasted_iota(jnp.int32, (devs, LANES), 1)
    holder, inner = row // SUB, row % SUB
    block = jnp.where(inner < own, holder * own + inner, -1)
    topk = chosen_ref.shape[3]
    across = lax.broadcasted_iota(jnp.int32, (count, count), 1)
    down = lax.broadcasted_iota(jnp.int32, (count, count), 0)
    lower = jnp.where((across // SUB == down // SUB) & (across < down), 1.0, 0.0).astype(BF)
    for s in range(seqs):
        seen = jnp.zeros((count, LANES), F32)
        named = []
        for b in range(own):
            hit = jnp.where(block[:, :topk] == chosen_ref[s, b], 1.0, 0.0)
            hit = jnp.broadcast_to(jnp.max(hit, axis=1, keepdims=True), (count, LANES))
            named_ref[s * own + b] = hit.reshape(devs, SUB, LANES)
            named.append(hit)
            seen = jnp.maximum(seen, hit)
        seen = jnp.where(holder < me, seen, 0.0)
        rank = jnp.dot(lower, seen.astype(BF), preferred_element_type=F32)
        for j in range(MOST):
            hot = jnp.where(rank == j, seen, 0.0)
            hot_ref[:, s, j] = hot.reshape(devs, SUB, LANES)
            oks = [jnp.sum((hot * n).reshape(devs, SUB, LANES), axis=1) for n in named]
            for t in range(pairs):
                ok = jnp.where(lane < BLK, oks[PAIR * t], oks[PAIR * t + 1])
                farb_ref[s * pairs + t, j] = (1.0 - ok) * NEG
        for t in range(pairs):
            ok = jnp.where(
                lane[:SUB] < BLK,
                named_ref[s * own + PAIR * t, me],
                named_ref[s * own + PAIR * t + 1, me],
            )
            nearb_ref[s * pairs + t] = (1.0 - ok) * NEG

    pl.semaphore_wait(barrier, devs - 1 + tps - 1)
    loop(0, me, lambda m: ask(m, me).start())

    for copy in ins[:3]:
        copy.wait()
    for s in range(seqs):
        near_ref[s] = jnp.concatenate([k_ref[s], v_ref[s]], axis=0).T
        gate_ref[s] = jax.nn.sigmoid(g_ref[s]).T

    def reply(s, i):
        n = devs - 1 - i
        for j in range(MOST):
            total = None
            for b in range(own):
                one = asked_ref[n, s, j, b : b + 1, :].astype(BF)
                term = one * near_ref[s, b * BLK : (b + 1) * BLK, :]
                total = term if total is None else total + term
            reply_ref[s, n, j * BLK : (j + 1) * BLK, :] = total
        answer(s, n, me).start()

    def first(i):
        ask(0, devs - 1 - i).wait_recv()
        reply(0, i)

    later = devs - 1 - me
    nearest = jnp.minimum(max(devs // 4, 1), later)
    loop(0, nearest, first)

    for t in peers:
        loop(0, groups, lambda g: shuffle(g, t, my_tp).start())
    loop(0, groups, lambda g: keep(g).start())

    for copy in ins[3:]:
        copy.wait()
    chunks = devs - 1
    span = SPAN * wide
    blocks = [(t, h) for t in range(pairs) for h in range(heads // SPAN)]
    dims = (((1,), (1,)), ((), ()))
    ahead = lax.broadcasted_iota(jnp.int32, (wide, span), 0) <= lax.rem(
        lax.broadcasted_iota(jnp.int32, (wide, span), 1), wide
    )

    def settle(s):
        def add(n):
            back(s, 0, n).wait_recv()
            for b in range(own):
                term = None
                for j in range(MOST):
                    one = asked_ref[n, s, j, b : b + 1, :]
                    more = one * back_ref[s, n, j * BLK : (j + 1) * BLK, :].astype(F32)
                    term = more if term is None else term + more
                total_ref[s, b * BLK : (b + 1) * BLK, :] += term

        loop(me + 1, devs, add)
        both = total_ref[s].T.astype(BF)
        kg_ref[s] = both[:hd]
        vo_ref[s] = both[hd:]
        vg_ref[s, at(my_tp, hd), :] = both[hd:]
        for t in peers:
            spread(s, t, my_tp).start()

    def score(s, kv, i, chunk, bias, diagonal, carry):
        top, norm, dot = carry
        cols = slice(i * span, (i + 1) * span)
        raw = lax.dot_general(kv, qs_ref[s, i], dims, preferred_element_type=F32) * log2e
        wg = lax.dot_general(kv, bg_ref[s, i], dims, preferred_element_type=F32)
        sc = jnp.concatenate(
            [
                raw[j * BLK : (j + 1) * BLK] + jnp.concatenate([b] * SPAN, axis=1)
                for j, b in enumerate(bias)
            ],
            axis=0,
        )
        if diagonal:
            sc = jnp.where(ahead, sc, NEG)
        peak = jnp.maximum(top, jnp.max(sc, axis=0, keepdims=True))
        p = jnp.exp2(sc - peak)
        less = jnp.exp2(top - peak)
        s_ref[chunk, :, cols] = p.astype(s_ref.dtype)
        w_ref[chunk, :, cols] = wg.astype(w_ref.dtype)
        top_ref[chunk, :, cols] = peak
        norm = norm * less + jnp.sum(p, axis=0, keepdims=True)
        dot = dot * less + jnp.sum(p * wg, axis=0, keepdims=True)
        return peak, norm, dot

    def setup(s):
        for t in range(pairs):
            tok = slice(t * wide, (t + 1) * wide)
            q = (q_ref[s, tok, :].astype(F32) * scale).astype(BF)
            cot = c_ref[s, tok, :].astype(F32)
            gate = gate_ref[s, tok, :]
            zero = jnp.zeros((span, hd), BF)
            for h in range(heads // SPAN):
                hs = range(h * SPAN, (h + 1) * SPAN)
                qs = jnp.concatenate([q[:, k * hd : (k + 1) * hd] for k in hs], axis=0)
                bg = jnp.concatenate(
                    [gate[:, k : k + 1] * cot[:, k * hd : (k + 1) * hd] for k in hs], axis=0
                ).astype(BF)
                i = t * (heads // SPAN) + h
                qs_ref[s, i] = jnp.concatenate([qs, zero], axis=1)
                bg_ref[s, i] = jnp.concatenate([zero, bg], axis=1)
        for i, (t, h) in enumerate(blocks):
            carry = (jnp.full((1, span), NEG, F32), jnp.zeros((1, span), F32), jnp.zeros((1, span), F32))
            for c in range(t, -1, -1):
                kv = near_ref[s, c * wide : (c + 1) * wide, :]
                bias = [
                    nearb_ref[s * pairs + t, c * PAIR + j : c * PAIR + j + 1, :] for j in range(PAIR)
                ]
                carry = score(s, kv, i, chunks + s * pairs + c, bias, c == t, carry)
            for k in range(3):
                run_ref[s, k, :, i * span : (i + 1) * span] = carry[k]

    def attention(s):
        carries = tuple(
            tuple(run_ref[s, k, :, i * span : (i + 1) * span] for k in range(3))
            for i in range(len(blocks))
        )

        def forth(i, carries):
            m = me - 1 - i
            answer(s, 0, m).wait_recv()
            kv = far_ref[s, m]
            return tuple(
                score(
                    s, kv, i, m,
                    [farb_ref[s * pairs + t, j, pl.ds(m, 1), :] for j in range(MOST)],
                    False, carries[i],
                )
                for i, (t, h) in enumerate(blocks)
            )

        carries = lax.fori_loop(0, me, forth, carries)

        @pl.when(s > 0)
        def _():
            settle(s - 1)

        tops = [carry[0] for carry in carries]
        invs = [1.0 / carry[1] for carry in carries]
        dots = [carry[2] * inv for carry, inv in zip(carries, invs)]
        dqt_ref[...] = jnp.zeros_like(dqt_ref)

        def grad(kv, chunk, first_t):
            kt = (kv[:, :hd] * scale).astype(BF).T
            total = None
            for i, (t, h) in enumerate(blocks):
                if t < first_t:
                    continue
                cols = slice(i * span, (i + 1) * span)
                part = jnp.exp2(top_ref[chunk, :, cols] - tops[i]) * invs[i]
                w = s_ref[chunk, :, cols].astype(F32) * part
                ds = (w * (w_ref[chunk, :, cols].astype(F32) - dots[i])).astype(BF)
                more = jnp.dot(ds, qs_ref[s, i], preferred_element_type=F32)
                more += jnp.dot(w.astype(BF), bg_ref[s, i], preferred_element_type=F32)
                total = more if total is None else total + more
                dqt_ref[:, cols] += jnp.dot(kt, ds, preferred_element_type=F32)
            return total

        def give(m):
            out_ref[s, m] = grad(far_ref[s, m], m, 0).astype(BF)
            back(s, m, me).start()

        loop(0, me, give)
        for c in range(pairs):
            kv = near_ref[s, c * wide : (c + 1) * wide, :]
            total_ref[s, c * wide : (c + 1) * wide, :] = grad(kv, chunks + s * pairs + c, c)
        for t in range(pairs):
            dqt = jnp.concatenate(
                [dqt_ref[:, (t * heads + h) * wide : (t * heads + h + 1) * wide] for h in range(heads)],
                axis=0,
            )
            dq_ref[s, t * wide : (t + 1) * wide, :] = dqt.T.astype(BF)

    setup(0)
    loop(nearest, later, first)
    for s in range(1, seqs):
        setup(s)
        loop(0, later, functools.partial(reply, s))
    loop(0, seqs, attention)
    puts = [put(0, dq_ref, dq_out)]
    puts[0].start()

    def product(s, g):
        return jnp.dot(vg_ref[s], rows_ref[g, s], preferred_element_type=F32)

    def begin():
        for t in peers:
            loop(0, groups, lambda g: shuffle(g, t, t).wait_recv())
        loop(0, groups, lambda g: keep(g).wait())
        for s in range(seqs - 1):
            for t in peers:
                spread(s, t, t).wait_recv()

            def early(g):
                if s == 0:
                    acc_ref[g] = product(s, g)
                else:
                    acc_ref[g] += product(s, g)

            loop(0, groups, early)

    settle(seqs - 1)
    begin()

    for out in [put(1, kg_ref, kg_out), put(2, vo_ref, vo_out)]:
        out.start()
        puts.append(out)
    for t in peers:
        spread(seqs - 1, t, t).wait_recv()

    def other(i):
        low = halves - 1 - i
        low = jnp.where(low > mine, low, low - 1)
        high = jnp.where(i < mine, i, i + 1)
        return jnp.where(i == halves - 1, mine, jnp.where(mine * 2 < halves, low, high))

    def final(g):
        last = product(seqs - 1, g)
        return last if seqs == 1 else last + acc_ref[g]

    if groups == devs:

        def stage(i):
            g = other(i)
            part_ref[g * DUO + 1 - my_u] = final(g * DUO + 1 - my_u).astype(BF)
            toss(g).start()

        loop(0, halves, stage)
    else:
        each = devs // groups

        def stage(g):
            part_ref[pl.ds(g * each, each)] = final(g).T.astype(BF).reshape((each,) + part_ref.shape[1:])

        loop(0, groups, stage)
        loop(0, halves, lambda i: toss(other(i)).start())

    def merge(i):
        g = other(i)
        if groups == devs:
            here = final(g * DUO + my_u)
        else:
            here = part_ref[g * DUO + my_u].astype(F32)
        toss(g).wait_recv()
        both_ref[g] = (here + mate_ref[g].astype(F32)).astype(BF)

        @pl.when(i < halves - 1)
        def _():
            piece(g, mine).start()

    loop(0, halves, merge)
    piece_ref[mine] = both_ref[mine]
    loop(0, halves - 1, lambda i: piece(other(i), other(i)).wait_recv())
    result = piece_ref[0].astype(F32)
    for n in range(1, halves):
        result += piece_ref[n].astype(F32)
    wg_ref[...] = result.T if groups == devs else result
    puts.append(put(3, wg_ref, wg_out))
    puts[-1].start()

    loop(0, me, lambda m: ask(m, me).wait_send())
    for t in peers:
        loop(0, groups, lambda g: shuffle(g, t, my_tp).wait_send())
    for s in range(seqs):
        loop(me + 1, devs, lambda n: answer(s, n, me).wait_send())
        loop(0, me, lambda m: back(s, m, me).wait_send())
        for t in peers:
            spread(s, t, my_tp).wait_send()
    loop(0, halves, lambda i: toss(i).wait_send())
    loop(0, halves - 1, lambda i: piece(other(i), mine).wait_send())
    for out in puts:
        out.wait()


def leave(count, *refs):
    ins, outs, held = refs[:count], refs[count : 2 * count], refs[2 * count : 3 * count]
    sems = refs[3 * count]
    reads = [pltpu.make_async_copy(ins[i], held[i], sems.at[0, i]) for i in range(count)]
    writes = [pltpu.make_async_copy(held[i], outs[i], sems.at[1, i]) for i in range(count)]
    for read in reads:
        read.start()
    for read, write in zip(reads, writes):
        read.wait()
        write.start()
    for write in writes:
        write.wait()


def on_device(queries, key_states, value_states, cotangent, gate_logits, layer_input, chosen):
    seqs, toks, width = queries.shape
    hd = key_states.shape[2]
    heads = width // hd
    own = toks // BLK
    pairs = own // PAIR
    devs = lax.axis_size("kv")
    tps = lax.axis_size("tp")
    pos = layer_input.shape[1]
    share = layer_input.shape[2] // (devs * tps)
    halves = devs // DUO
    groups, cut = devs, share
    if share % LANES:
        groups, cut = devs * share // LANES, LANES
        layer_input = layer_input.reshape(seqs, pos, devs, tps, share)
        layer_input = jnp.swapaxes(layer_input, 2, 3).reshape(seqs, pos, devs * tps * share)
    part = (tps * hd, share) if groups == devs else (share, tps * hd)
    chunks = devs - 1 + seqs * pairs
    rows = heads * PAIR * BLK
    scores = (chunks, PAIR * BLK, pairs * rows)
    sent = (MOST * BLK, 2 * hd)

    vmem = pl.BlockSpec(memory_space=pltpu.VMEM)
    hbm = pl.BlockSpec(memory_space=pl.ANY)
    dma = pltpu.SemaphoreType.DMA
    results = pl.pallas_call(
        functools.partial(whole, devs, tps, seqs, own, heads, hd, cut, groups),
        in_specs=[vmem] + [hbm] * 6,
        out_specs=[hbm] * 4,
        out_shape=[
            jax.ShapeDtypeStruct((seqs, toks, width), BF),
            jax.ShapeDtypeStruct((seqs, hd, toks), BF),
            jax.ShapeDtypeStruct((seqs, hd, toks), BF),
            jax.ShapeDtypeStruct((share, tps * hd), F32),
        ],
        scratch_shapes=[
            pltpu.VMEM((seqs, toks, width), BF),
            pltpu.VMEM((seqs, toks, width), BF),
            pltpu.VMEM((seqs, heads, toks), F32),
            pltpu.VMEM((seqs, hd, toks), BF),
            pltpu.VMEM((seqs, hd, toks), BF),
            pltpu.VMEM((seqs, toks, width), BF),
            pltpu.VMEM((seqs, hd, toks), BF),
            pltpu.VMEM((seqs, hd, toks), BF),
            pltpu.VMEM((share, tps * hd), F32),
            pltpu.VMEM((seqs, toks, 2 * hd), BF),
            pltpu.VMEM((seqs, toks, heads), F32),
            pltpu.VMEM((seqs * own, devs, SUB, LANES), F32),
            pltpu.VMEM((devs, seqs, MOST, SUB, LANES), F32),
            pltpu.VMEM((devs, seqs, MOST, SUB, LANES), F32),
            pltpu.VMEM((seqs * pairs, MOST, devs, LANES), F32),
            pltpu.VMEM((seqs * pairs, SUB, LANES), F32),
            pltpu.VMEM((seqs, devs) + sent, BF),
            pltpu.VMEM((seqs, devs - 1) + sent, BF),
            pltpu.VMEM((groups, seqs, toks, cut), BF),
            pltpu.VMEM((seqs, pairs * heads // SPAN, SPAN * PAIR * BLK, 2 * hd), BF),
            pltpu.VMEM((seqs, pairs * heads // SPAN, SPAN * PAIR * BLK, 2 * hd), BF),
            pltpu.VMEM(scores, F32 if math.prod(scores) <= 5 * 2**20 else BF),
            pltpu.VMEM(scores, F32 if math.prod(scores) <= 5 * 2**20 else BF),
            pltpu.VMEM((chunks, 1, pairs * rows), F32),
            pltpu.VMEM((seqs, 3, 1, pairs * rows), F32),
            pltpu.VMEM((hd, pairs * rows), F32),
            pltpu.VMEM((seqs, devs - 1) + sent, BF),
            pltpu.VMEM((seqs, toks, 2 * hd), F32),
            pltpu.VMEM((seqs, devs) + sent, BF),
            pltpu.VMEM((seqs, tps * hd, toks), BF),
            pltpu.VMEM((groups, tps * hd, cut), F32),
            pltpu.VMEM((devs,) + part, BF),
            pltpu.VMEM((halves,) + part, BF),
            pltpu.VMEM((halves,) + part, BF),
            pltpu.VMEM((halves,) + part, BF),
            dma((devs,)), dma((devs,)),
            dma((seqs, devs)), dma((seqs, devs)),
            dma((tps, groups)), dma((tps, groups)), dma((groups,)),
            dma((seqs, devs)), dma((seqs, devs)),
            dma((seqs, tps)), dma((seqs, tps)),
            dma((halves,)), dma((halves,)),
            dma((halves,)), dma((halves,)),
            dma((5,)), dma((4,)),
        ],
        compiler_params=pltpu.CompilerParams(
            collective_id=0, has_side_effects=True, vmem_limit_bytes=60 * 2**20
        ),
    )(
        chosen, queries, cotangent, jnp.swapaxes(gate_logits, 1, 2),
        jnp.swapaxes(key_states, 1, 2), jnp.swapaxes(value_states, 1, 2), layer_input,
    )
    query_grad, key_grad, value_grad, weight_grad = pl.pallas_call(
        functools.partial(leave, len(results)),
        in_specs=[hbm] * len(results),
        out_specs=[hbm] * len(results),
        out_shape=[jax.ShapeDtypeStruct(r.shape, r.dtype) for r in results],
        scratch_shapes=[pltpu.VMEM(r.shape, r.dtype) for r in results] + [dma((2, len(results)))],
        compiler_params=pltpu.CompilerParams(vmem_limit_bytes=60 * 2**20),
    )(*results)
    return query_grad, jnp.swapaxes(key_grad, 1, 2), jnp.swapaxes(value_grad, 1, 2), weight_grad


def solution(mesh):
    in_specs = (
        P(None, "kv", "tp"),
        P(None, "kv", "tp"),
        P(None, "kv", "tp"),
        P(None, "kv", "tp"),
        P(None, "kv", "tp"),
        P(None, ("kv", "tp"), None),
        P(None, "kv", "tp", None),
    )
    out_specs = (
        P(None, "kv", "tp"),
        P(None, "kv", "tp"),
        P(None, "kv", "tp"),
        P(("kv", "tp"), None),
    )
    return jax.shard_map(
        on_device, mesh=mesh, in_specs=in_specs, out_specs=out_specs, check_vma=False
    )
```

```python
import functools
import math

import jax
import jax.numpy as jnp
from jax import lax
from jax.experimental import pallas as pl
from jax.experimental.pallas import tpu as pltpu
from jax.sharding import PartitionSpec as P

BLK = 64
MOST = 2
PAIR = 2
DUO = 2
SUB = 8
LANES = 128
SPAN = 2
NEG = -1e30
MESH = pl.DeviceIdType.MESH
BF = jnp.bfloat16
F32 = jnp.float32


def loop(lo, hi, body):
    def step(i, carry):
        body(i)
        return carry

    lax.fori_loop(lo, hi, step, 0)


def at(i, size):
    return pl.ds(i * size, size) if isinstance(i, int) else pl.ds(pl.multiple_of(i * size, size), size)


def whole(
    devs, tps, seqs, own, heads, hd, share, groups, defer,
    chosen_ref, q_in, c_in, g_in, k_in, v_in, li_ref,
    dq_out, kg_out, vo_out, wg_out,
    q_ref, c_ref, g_ref, k_ref, v_ref, dq_ref, kg_ref, vo_ref, wg_ref,
    near_ref, gate_ref, named_ref, hot_ref, asked_ref, farb_ref, nearb_ref,
    reply_ref, far_ref, rows_ref, qs_ref, bg_ref, s_ref, w_ref, ds_ref, top_ref, run_ref, dqt_ref,
    out_ref, total_ref, back_ref, vg_ref, acc_ref, part_ref, mate_ref, both_ref, piece_ref,
    hot_send, hot_recv, far_send, far_recv, li_send, li_recv, li_sem,
    back_send, back_recv, vg_send, vg_recv, toss_send, toss_recv, piece_send, piece_recv, in_sem, out_sem,
):
    me = lax.axis_index("kv")
    my_tp = lax.axis_index("tp")
    toks = own * BLK
    pos = li_ref.shape[1]
    pairs = own // PAIR
    wide = PAIR * BLK
    far_rows = MOST * BLK
    scale = hd**-0.5
    log2e = math.log2(math.e)

    barrier = pltpu.get_barrier_semaphore()
    loop(1, devs, lambda d: pl.semaphore_signal(
        barrier, inc=1, device_id={"kv": lax.rem(me + d, devs)}, device_id_type=MESH
    ))
    for d in range(1, tps):
        pl.semaphore_signal(
            barrier, inc=1, device_id={"tp": lax.rem(my_tp + d, tps)}, device_id_type=MESH
        )

    def ask(m, src):
        return pltpu.make_async_remote_copy(
            src_ref=hot_ref.at[m], dst_ref=asked_ref.at[src],
            send_sem=hot_send.at[m], recv_sem=hot_recv.at[src],
            device_id={"kv": m}, device_id_type=MESH,
        )

    def answer(s, n, src):
        return pltpu.make_async_remote_copy(
            src_ref=reply_ref.at[s, n], dst_ref=far_ref.at[s, src],
            send_sem=far_send.at[s, n], recv_sem=far_recv.at[s, src],
            device_id={"kv": n}, device_id_type=MESH,
        )

    def columns(g, t):
        return at(g * tps + t if groups == devs else t * groups + g, share)

    def shuffle(g, t, src):
        return pltpu.make_async_remote_copy(
            src_ref=li_ref.at[:, :, columns(g, t)],
            dst_ref=rows_ref.at[g, :, at(src, pos), :],
            send_sem=li_send.at[t, g], recv_sem=li_recv.at[src, g],
            device_id={"tp": t}, device_id_type=MESH,
        )

    def keep(g):
        return pltpu.make_async_copy(
            li_ref.at[:, :, columns(g, my_tp)], rows_ref.at[g, :, at(my_tp, pos), :], li_sem.at[g]
        )

    def back(s, m, src):
        return pltpu.make_async_remote_copy(
            src_ref=out_ref.at[s, m], dst_ref=back_ref.at[s, src],
            send_sem=back_send.at[s, m], recv_sem=back_recv.at[s, src],
            device_id={"kv": m}, device_id_type=MESH,
        )

    def spread(s, t, src):
        return pltpu.make_async_remote_copy(
            src_ref=vg_ref.at[s, at(src, hd), :], dst_ref=vg_ref.at[s, at(src, hd), :],
            send_sem=vg_send.at[s, t], recv_sem=vg_recv.at[s, src],
            device_id={"tp": t}, device_id_type=MESH,
        )

    halves, mine, my_u = devs // DUO, me // DUO, me % DUO

    def toss(g):
        return pltpu.make_async_remote_copy(
            src_ref=part_ref.at[g * DUO + 1 - my_u], dst_ref=mate_ref.at[g],
            send_sem=toss_send.at[g], recv_sem=toss_recv.at[g],
            device_id={"kv": me + 1 - 2 * my_u}, device_id_type=MESH,
        )

    def piece(g, src):
        return pltpu.make_async_remote_copy(
            src_ref=both_ref.at[g], dst_ref=piece_ref.at[src],
            send_sem=piece_send.at[g], recv_sem=piece_recv.at[src],
            device_id={"kv": g * DUO + my_u}, device_id_type=MESH,
        )

    ins = [
        pltpu.make_async_copy(src, dst, in_sem.at[i])
        for i, (src, dst) in enumerate(
            [(k_in, k_ref), (v_in, v_ref), (g_in, g_ref), (q_in, q_ref), (c_in, c_ref)]
        )
    ]
    for copy in ins:
        copy.start()

    def put(i, src, dst):
        return pltpu.make_async_copy(src, dst, out_sem.at[i])

    peers = [lax.rem(my_tp + d, tps) for d in range(1, tps)]

    count = devs * SUB
    row = lax.broadcasted_iota(jnp.int32, (count, LANES), 0)
    lane = lax.broadcasted_iota(jnp.int32, (devs, LANES), 1)
    holder, inner = row // SUB, row % SUB
    block = jnp.where(inner < own, holder * own + inner, -1)
    topk = chosen_ref.shape[3]
    across = lax.broadcasted_iota(jnp.int32, (count, count), 1)
    down = lax.broadcasted_iota(jnp.int32, (count, count), 0)
    lower = jnp.where((across // SUB == down // SUB) & (across < down), 1.0, 0.0).astype(BF)
    for s in range(seqs):
        seen = jnp.zeros((count, LANES), F32)
        named = []
        for b in range(own):
            hit = jnp.where(block[:, :topk] == chosen_ref[s, b], 1.0, 0.0)
            hit = jnp.broadcast_to(jnp.max(hit, axis=1, keepdims=True), (count, LANES))
            named_ref[s * own + b] = hit.reshape(devs, SUB, LANES)
            named.append(hit)
            seen = jnp.maximum(seen, hit)
        seen = jnp.where(holder < me, seen, 0.0)
        rank = jnp.dot(lower, seen.astype(BF), preferred_element_type=F32)
        for j in range(MOST):
            hot = jnp.where(rank == j, seen, 0.0)
            hot_ref[:, s, j] = hot.reshape(devs, SUB, LANES)
            oks = [jnp.sum((hot * n).reshape(devs, SUB, LANES), axis=1) for n in named]
            for t in range(pairs):
                ok = jnp.where(lane < BLK, oks[PAIR * t], oks[PAIR * t + 1])
                farb_ref[s * pairs + t, j] = (1.0 - ok) * NEG
        for t in range(pairs):
            ok = jnp.where(
                lane[:SUB] < BLK,
                named_ref[s * own + PAIR * t, me],
                named_ref[s * own + PAIR * t + 1, me],
            )
            nearb_ref[s * pairs + t] = (1.0 - ok) * NEG

    pl.semaphore_wait(barrier, devs - 1 + tps - 1)
    loop(0, me, lambda m: ask(m, me).start())

    for copy in ins[:3]:
        copy.wait()
    for s in range(seqs):
        near_ref[s] = jnp.concatenate([k_ref[s], v_ref[s]], axis=0).T
        gate_ref[s] = jax.nn.sigmoid(g_ref[s]).T

    def reply(s, i):
        n = devs - 1 - i
        for j in range(MOST):
            total = None
            for b in range(own):
                one = asked_ref[n, s, j, b : b + 1, :].astype(BF)
                term = one * near_ref[s, b * BLK : (b + 1) * BLK, :]
                total = term if total is None else total + term
            reply_ref[s, n, j * BLK : (j + 1) * BLK, :] = total
        answer(s, n, me).start()

    def first(i):
        ask(0, devs - 1 - i).wait_recv()
        reply(0, i)

    later = devs - 1 - me
    nearest = jnp.minimum(max(devs // 4, 1), later)
    loop(0, nearest, first)

    for t in peers:
        loop(0, groups, lambda g: shuffle(g, t, my_tp).start())
    loop(0, groups, lambda g: keep(g).start())

    for copy in ins[3:]:
        copy.wait()
    chunks = devs - 1
    span = SPAN * wide
    blocks = [(t, h) for t in range(pairs) for h in range(heads // SPAN)]
    dims = (((1,), (1,)), ((), ()))
    ahead = lax.broadcasted_iota(jnp.int32, (wide, span), 0) <= lax.rem(
        lax.broadcasted_iota(jnp.int32, (wide, span), 1), wide
    )

    def settle(s):
        def add(n):
            back(s, 0, n).wait_recv()
            for b in range(own):
                term = None
                for j in range(MOST):
                    one = asked_ref[n, s, j, b : b + 1, :]
                    more = one * back_ref[s, n, j * BLK : (j + 1) * BLK, :].astype(F32)
                    term = more if term is None else term + more
                total_ref[s, b * BLK : (b + 1) * BLK, :] += term

        loop(me + 1, devs, add)
        both = total_ref[s].T.astype(BF)
        kg_ref[s] = both[:hd]
        vo_ref[s] = both[hd:]
        vg_ref[s, at(my_tp, hd), :] = both[hd:]
        for t in peers:
            spread(s, t, my_tp).start()

    def score(s, kv, i, chunk, bias, diagonal, carry):
        top, norm, dot = carry
        cols = slice(i * span, (i + 1) * span)
        raw = lax.dot_general(kv, qs_ref[s, i], dims, preferred_element_type=F32) * log2e
        wg = lax.dot_general(kv, bg_ref[s, i], dims, preferred_element_type=F32)
        sc = jnp.concatenate(
            [
                raw[j * BLK : (j + 1) * BLK] + jnp.concatenate([b] * SPAN, axis=1)
                for j, b in enumerate(bias)
            ],
            axis=0,
        )
        if diagonal:
            sc = jnp.where(ahead, sc, NEG)
        peak = jnp.maximum(top, jnp.max(sc, axis=0, keepdims=True))
        p = jnp.exp2(sc - peak)
        less = jnp.exp2(top - peak)
        s_ref[chunk, :, cols] = p.astype(s_ref.dtype)
        w_ref[chunk, :, cols] = wg.astype(w_ref.dtype)
        top_ref[chunk, :, cols] = peak
        norm = norm * less + jnp.sum(p, axis=0, keepdims=True)
        dot = dot * less + jnp.sum(p * wg, axis=0, keepdims=True)
        return peak, norm, dot

    def setup(s):
        for t in range(pairs):
            tok = slice(t * wide, (t + 1) * wide)
            q = (q_ref[s, tok, :].astype(F32) * scale).astype(BF)
            cot = c_ref[s, tok, :].astype(F32)
            gate = gate_ref[s, tok, :]
            zero = jnp.zeros((span, hd), BF)
            for h in range(heads // SPAN):
                hs = range(h * SPAN, (h + 1) * SPAN)
                qs = jnp.concatenate([q[:, k * hd : (k + 1) * hd] for k in hs], axis=0)
                bg = jnp.concatenate(
                    [gate[:, k : k + 1] * cot[:, k * hd : (k + 1) * hd] for k in hs], axis=0
                ).astype(BF)
                i = t * (heads // SPAN) + h
                qs_ref[s, i] = jnp.concatenate([qs, zero], axis=1)
                bg_ref[s, i] = jnp.concatenate([zero, bg], axis=1)
        for i, (t, h) in enumerate(blocks):
            carry = (jnp.full((1, span), NEG, F32), jnp.zeros((1, span), F32), jnp.zeros((1, span), F32))
            for c in range(t, -1, -1):
                kv = near_ref[s, c * wide : (c + 1) * wide, :]
                bias = [
                    nearb_ref[s * pairs + t, c * PAIR + j : c * PAIR + j + 1, :] for j in range(PAIR)
                ]
                carry = score(s, kv, i, chunks + s * pairs + c, bias, c == t, carry)
            for k in range(3):
                run_ref[s, k, :, i * span : (i + 1) * span] = carry[k]

    def attention(s):
        carries = tuple(
            tuple(run_ref[s, k, :, i * span : (i + 1) * span] for k in range(3))
            for i in range(len(blocks))
        )

        def forth(i, carries):
            m = me - 1 - i
            answer(s, 0, m).wait_recv()
            kv = far_ref[s, m]
            return tuple(
                score(
                    s, kv, i, m,
                    [farb_ref[s * pairs + t, j, pl.ds(m, 1), :] for j in range(MOST)],
                    False, carries[i],
                )
                for i, (t, h) in enumerate(blocks)
            )

        carries = lax.fori_loop(0, me, forth, carries)

        @pl.when(s > 0)
        def _():
            settle(s - 1)

        tops = [carry[0] for carry in carries]
        invs = [1.0 / carry[1] for carry in carries]
        dots = [carry[2] * inv for carry, inv in zip(carries, invs)]
        if not defer:
            dqt_ref[...] = jnp.zeros_like(dqt_ref)

        def grad(kv, chunk, slot, first_t):
            kt = None if defer else (kv[:, :hd] * scale).astype(BF).T
            total = None
            for i, (t, h) in enumerate(blocks):
                if t < first_t:
                    continue
                cols = slice(i * span, (i + 1) * span)
                part = jnp.exp2(top_ref[chunk, :, cols] - tops[i]) * invs[i]
                w = s_ref[chunk, :, cols].astype(F32) * part
                ds = (w * (w_ref[chunk, :, cols].astype(F32) - dots[i])).astype(BF)
                more = jnp.dot(ds, qs_ref[s, i], preferred_element_type=F32)
                more += jnp.dot(w.astype(BF), bg_ref[s, i], preferred_element_type=F32)
                total = more if total is None else total + more
                if defer:
                    ds_ref[slot, :, cols] = ds
                else:
                    dqt_ref[:, cols] += jnp.dot(kt, ds, preferred_element_type=F32)
            return total

        def give(i):
            m = jnp.where(me < 2 * quarter, i, order(i))
            out_ref[s, m] = grad(far_ref[s, m], m, s * (chunks + pairs) + m, 0).astype(BF)
            back(s, m, me).start()

        loop(0, me, give)
        for c in range(pairs):
            kv = near_ref[s, c * wide : (c + 1) * wide, :]
            total_ref[s, c * wide : (c + 1) * wide, :] = grad(
                kv, chunks + s * pairs + c, s * (chunks + pairs) + chunks + c, c
            )
        if not defer:
            turn(s)

    quarter = devs // 4

    def order(i):
        return jnp.where(i < quarter, i + quarter, jnp.where(i < 2 * quarter, i - quarter, i))

    def turn(s):
        for t in range(pairs):
            dqt = jnp.concatenate(
                [dqt_ref[:, (t * heads + h) * wide : (t * heads + h + 1) * wide] for h in range(heads)],
                axis=0,
            )
            dq_ref[s, t * wide : (t + 1) * wide, :] = dqt.T.astype(BF)

    def query_side(s):
        first = s * (chunks + pairs)
        for c in range(pairs):
            kt = (near_ref[s, c * wide : (c + 1) * wide, :hd] * scale).astype(BF).T
            for i, (t, h) in enumerate(blocks):
                if t >= c:
                    cols = slice(i * span, (i + 1) * span)
                    more = jnp.dot(kt, ds_ref[first + chunks + c, :, cols], preferred_element_type=F32)
                    if c == 0:
                        dqt_ref[:, cols] = more
                    else:
                        dqt_ref[:, cols] += more

        def far_side(m):
            kt = (far_ref[s, m][:, :hd] * scale).astype(BF).T
            for i in range(len(blocks)):
                cols = slice(i * span, (i + 1) * span)
                dqt_ref[:, cols] += jnp.dot(kt, ds_ref[first + m, :, cols], preferred_element_type=F32)

        loop(0, me, far_side)
        turn(s)

    setup(0)
    loop(nearest, later, first)
    for s in range(1, seqs):
        setup(s)
        loop(0, later, functools.partial(reply, s))
    loop(0, seqs, attention)
    puts = []

    def product(s, g):
        return jnp.dot(vg_ref[s], rows_ref[g, s], preferred_element_type=F32)

    def begin():
        for t in peers:
            loop(0, groups, lambda g: shuffle(g, t, t).wait_recv())
        loop(0, groups, lambda g: keep(g).wait())
        for s in range(seqs - 1):
            for t in peers:
                spread(s, t, t).wait_recv()

            def early(g):
                if s == 0:
                    acc_ref[g] = product(s, g)
                else:
                    acc_ref[g] += product(s, g)

            loop(0, groups, early)

    settle(seqs - 1)
    begin()

    for out in [put(1, kg_ref, kg_out), put(2, vo_ref, vo_out)]:
        out.start()
        puts.append(out)
    for t in peers:
        spread(seqs - 1, t, t).wait_recv()

    def other(i):
        low = halves - 1 - i
        low = jnp.where(low > mine, low, low - 1)
        high = jnp.where(i < mine, i, i + 1)
        return jnp.where(i == halves - 1, mine, jnp.where(mine * 2 < halves, low, high))

    def final(g):
        last = product(seqs - 1, g)
        return last if seqs == 1 else last + acc_ref[g]

    if groups == devs:

        def stage(i):
            g = other(i)
            part_ref[g * DUO + 1 - my_u] = final(g * DUO + 1 - my_u).astype(BF)
            toss(g).start()

        loop(0, halves, stage)
    else:
        each = devs // groups

        def stage(g):
            part_ref[pl.ds(g * each, each)] = final(g).T.astype(BF).reshape((each,) + part_ref.shape[1:])

        loop(0, groups, stage)
        loop(0, halves, lambda i: toss(other(i)).start())

    def merge(i):
        g = other(i)
        if groups == devs:
            here = final(g * DUO + my_u)
        else:
            here = part_ref[g * DUO + my_u].astype(F32)
        toss(g).wait_recv()
        both_ref[g] = (here + mate_ref[g].astype(F32)).astype(BF)

        @pl.when(i < halves - 1)
        def _():
            piece(g, mine).start()

    if defer:
        loop(0, seqs, query_side)
    puts.append(put(0, dq_ref, dq_out))
    puts[-1].start()
    loop(0, halves, merge)
    piece_ref[mine] = both_ref[mine]
    loop(0, halves - 1, lambda i: piece(other(i), other(i)).wait_recv())
    result = piece_ref[0].astype(F32)
    for n in range(1, halves):
        result += piece_ref[n].astype(F32)
    wg_ref[...] = result.T if groups == devs else result
    puts.append(put(3, wg_ref, wg_out))
    puts[-1].start()

    loop(0, me, lambda m: ask(m, me).wait_send())
    for t in peers:
        loop(0, groups, lambda g: shuffle(g, t, my_tp).wait_send())
    for s in range(seqs):
        loop(me + 1, devs, lambda n: answer(s, n, me).wait_send())
        loop(0, me, lambda m: back(s, m, me).wait_send())
        for t in peers:
            spread(s, t, my_tp).wait_send()
    loop(0, halves, lambda i: toss(i).wait_send())
    loop(0, halves - 1, lambda i: piece(other(i), mine).wait_send())
    for out in puts:
        out.wait()


def leave(count, *refs):
    ins, outs, held = refs[:count], refs[count : 2 * count], refs[2 * count : 3 * count]
    sems = refs[3 * count]
    reads = [pltpu.make_async_copy(ins[i], held[i], sems.at[0, i]) for i in range(count)]
    writes = [pltpu.make_async_copy(held[i], outs[i], sems.at[1, i]) for i in range(count)]
    for read in reads:
        read.start()
    for read, write in zip(reads, writes):
        read.wait()
        write.start()
    for write in writes:
        write.wait()


def on_device(queries, key_states, value_states, cotangent, gate_logits, layer_input, chosen):
    seqs, toks, width = queries.shape
    hd = key_states.shape[2]
    heads = width // hd
    own = toks // BLK
    pairs = own // PAIR
    devs = lax.axis_size("kv")
    tps = lax.axis_size("tp")
    pos = layer_input.shape[1]
    share = layer_input.shape[2] // (devs * tps)
    halves = devs // DUO
    groups, cut = devs, share
    if share % LANES:
        groups, cut = devs * share // LANES, LANES
        layer_input = layer_input.reshape(seqs, pos, devs, tps, share)
        layer_input = jnp.swapaxes(layer_input, 2, 3).reshape(seqs, pos, devs * tps * share)
    part = (tps * hd, share) if groups == devs else (share, tps * hd)
    chunks = devs - 1 + seqs * pairs
    rows = heads * PAIR * BLK
    scores = (chunks, PAIR * BLK, pairs * rows)
    kept = (seqs * (devs - 1 + pairs),) + scores[1:]
    defer = math.prod(kept) <= 5 * 2**20
    sent = (MOST * BLK, 2 * hd)

    vmem = pl.BlockSpec(memory_space=pltpu.VMEM)
    hbm = pl.BlockSpec(memory_space=pl.ANY)
    dma = pltpu.SemaphoreType.DMA
    results = pl.pallas_call(
        functools.partial(whole, devs, tps, seqs, own, heads, hd, cut, groups, defer),
        in_specs=[vmem] + [hbm] * 6,
        out_specs=[hbm] * 4,
        out_shape=[
            jax.ShapeDtypeStruct((seqs, toks, width), BF),
            jax.ShapeDtypeStruct((seqs, hd, toks), BF),
            jax.ShapeDtypeStruct((seqs, hd, toks), BF),
            jax.ShapeDtypeStruct((share, tps * hd), F32),
        ],
        scratch_shapes=[
            pltpu.VMEM((seqs, toks, width), BF),
            pltpu.VMEM((seqs, toks, width), BF),
            pltpu.VMEM((seqs, heads, toks), F32),
            pltpu.VMEM((seqs, hd, toks), BF),
            pltpu.VMEM((seqs, hd, toks), BF),
            pltpu.VMEM((seqs, toks, width), BF),
            pltpu.VMEM((seqs, hd, toks), BF),
            pltpu.VMEM((seqs, hd, toks), BF),
            pltpu.VMEM((share, tps * hd), F32),
            pltpu.VMEM((seqs, toks, 2 * hd), BF),
            pltpu.VMEM((seqs, toks, heads), F32),
            pltpu.VMEM((seqs * own, devs, SUB, LANES), F32),
            pltpu.VMEM((devs, seqs, MOST, SUB, LANES), F32),
            pltpu.VMEM((devs, seqs, MOST, SUB, LANES), F32),
            pltpu.VMEM((seqs * pairs, MOST, devs, LANES), F32),
            pltpu.VMEM((seqs * pairs, SUB, LANES), F32),
            pltpu.VMEM((seqs, devs) + sent, BF),
            pltpu.VMEM((seqs, devs - 1) + sent, BF),
            pltpu.VMEM((groups, seqs, toks, cut), BF),
            pltpu.VMEM((seqs, pairs * heads // SPAN, SPAN * PAIR * BLK, 2 * hd), BF),
            pltpu.VMEM((seqs, pairs * heads // SPAN, SPAN * PAIR * BLK, 2 * hd), BF),
            pltpu.VMEM(scores, F32 if math.prod(scores) <= 5 * 2**20 else BF),
            pltpu.VMEM(scores, F32 if math.prod(scores) <= 5 * 2**20 else BF),
            pltpu.VMEM(kept if defer else (1, SUB, LANES), BF),
            pltpu.VMEM((chunks, 1, pairs * rows), F32),
            pltpu.VMEM((seqs, 3, 1, pairs * rows), F32),
            pltpu.VMEM((hd, pairs * rows), F32),
            pltpu.VMEM((seqs, devs - 1) + sent, BF),
            pltpu.VMEM((seqs, toks, 2 * hd), F32),
            pltpu.VMEM((seqs, devs) + sent, BF),
            pltpu.VMEM((seqs, tps * hd, toks), BF),
            pltpu.VMEM((groups, tps * hd, cut), F32),
            pltpu.VMEM((devs,) + part, BF),
            pltpu.VMEM((halves,) + part, BF),
            pltpu.VMEM((halves,) + part, BF),
            pltpu.VMEM((halves,) + part, BF),
            dma((devs,)), dma((devs,)),
            dma((seqs, devs)), dma((seqs, devs)),
            dma((tps, groups)), dma((tps, groups)), dma((groups,)),
            dma((seqs, devs)), dma((seqs, devs)),
            dma((seqs, tps)), dma((seqs, tps)),
            dma((halves,)), dma((halves,)),
            dma((halves,)), dma((halves,)),
            dma((5,)), dma((4,)),
        ],
        compiler_params=pltpu.CompilerParams(
            collective_id=0, has_side_effects=True, vmem_limit_bytes=60 * 2**20
        ),
    )(
        chosen, queries, cotangent, jnp.swapaxes(gate_logits, 1, 2),
        jnp.swapaxes(key_states, 1, 2), jnp.swapaxes(value_states, 1, 2), layer_input,
    )
    query_grad, key_grad, value_grad, weight_grad = pl.pallas_call(
        functools.partial(leave, len(results)),
        in_specs=[hbm] * len(results),
        out_specs=[hbm] * len(results),
        out_shape=[jax.ShapeDtypeStruct(r.shape, r.dtype) for r in results],
        scratch_shapes=[pltpu.VMEM(r.shape, r.dtype) for r in results] + [dma((2, len(results)))],
        compiler_params=pltpu.CompilerParams(vmem_limit_bytes=60 * 2**20),
    )(*results)
    return query_grad, jnp.swapaxes(key_grad, 1, 2), jnp.swapaxes(value_grad, 1, 2), weight_grad


def solution(mesh):
    in_specs = (
        P(None, "kv", "tp"),
        P(None, "kv", "tp"),
        P(None, "kv", "tp"),
        P(None, "kv", "tp"),
        P(None, "kv", "tp"),
        P(None, ("kv", "tp"), None),
        P(None, "kv", "tp", None),
    )
    out_specs = (
        P(None, "kv", "tp"),
        P(None, "kv", "tp"),
        P(None, "kv", "tp"),
        P(("kv", "tp"), None),
    )
    return jax.shard_map(
        on_device, mesh=mesh, in_specs=in_specs, out_specs=out_specs, check_vma=False
    )
```
